32 devices in a mesh: sp: 8 (over z, x), tp: 4 (over y, core).
Axes of the slice: x: 2, y: 2, z: 4, core: 2. Of those that a mesh axis runs over, the one named last changes fastest.
Arguments:
- stream_in: bfloat16 [2048, 2048], P(('sp', 'tp')), may hold values from -6 to 6
- queries: bfloat16 [2048, 4096], P('sp', 'tp'), may hold values from -6 to 6
- key_rows: bfloat16 [2048, 4096], P('sp', 'tp'), may hold values from -6 to 6
- values: bfloat16 [2048, 8192], P('sp', 'tp'), may hold values from -6 to 6
- decay_low: bfloat16 [2048, 16], P('sp'), may hold values from -4 to 4
- decay_matrix: bfloat16 [16, 4096], P(None, 'tp'), may hold values from -1.5 to 1.5
- decay_bias: float32 [4096], P('tp')
- decay_shift: float32 [2048, 16], P('sp', 'tp'), may hold values from -1 to 0
- head_gain: float32 [512], replicated, may hold values from 0.1 to 1.9
- output_matrix: bfloat16 [8192, 2048], P('tp'), may hold values from -0.0625 to 0.0625
- feed_gain: float32 [2048], replicated, may hold values from 0.1 to 1.9
- routes: int32 [2048, 2], P('sp'), may hold values from 0 to 7, all different within a row; in each aligned block of 256 rows (0 to 255, 256 to 511, ...) at most 64 rows name the same one
- route_weights: float32 [2048, 2], P('sp'), may hold values from 0.2 to 1
- expert_gate: bfloat16 [8, 2048, 2816], P('sp', None, 'tp'), may hold values from -0.125 to 0.125
- specialist_widen: bfloat16 [8, 2048, 2816], P('sp', None, 'tp'), may hold values from -0.125 to 0.125
- expert_down: bfloat16 [8, 2816, 2048], P('sp', 'tp'), may hold values from -0.109375 to 0.109375
Outputs:
- layer_out: bfloat16 [2048, 2048], P(('sp', 'tp'))
The draws below stay inside these ranges and needn't reach their ends.
Inputs may be any that keep to these rules, and one draw needn't show every extreme that they name: `routes`: each row names 2 different experts; within each aligned block of 256 rows no expert is named by more than 64 rows, and in every draw some expert is named by exactly 64 rows of some block.
All inputs are finite; a program needn't handle non-finite values.
Results may differ from the reference program's by a relative error of at most 0.02.
Values may be sent and summed in bfloat16 or wider, within the bound.
A program may use at most 128 MiB of HBM per device.

```python
import math
import jax
import jax.numpy as jnp
import numpy as np
from jax import lax

D = 2048
HEADS = 16
HK = 256
HV = 512
RANK = 16
FF = 2816
TOP = 2
BLK = 128
TOK_DEV = 256
SEQUENCE_LENGTH = 2048
EXPERTS = 8
CAPG = 64
N_SP = 8
N_TP = 4


def draw_decay_bias(key, part):
    key_pick = jax.random.fold_in(key, 11)
    key_slow = jax.random.fold_in(key, 12)
    key_fast = jax.random.fold_in(key, 13)
    fast_heads = jax.random.uniform(key_pick, (HEADS,), jnp.float32) < 0.5
    slow_values = jnp.log(jnp.float32(SEQUENCE_LENGTH)) + 1.0 + jax.random.uniform(key_slow, (HEADS, HK), jnp.float32, 0.0, 1.5)
    fast_values = jax.random.uniform(key_fast, (HEADS, HK), jnp.float32, -0.5, 1.0)
    return jnp.where(fast_heads[:, None], fast_values, slow_values).reshape(HEADS * HK).astype(jnp.float32)


def draw_decay_shift(key, part):
    key_rate = jax.random.fold_in(key, 21)
    key_where = jax.random.fold_in(key, 22)
    key_loss = jax.random.fold_in(key, 23)
    blocks = SEQUENCE_LENGTH // TOK_DEV
    rates = jnp.exp(jax.random.uniform(key_rate, (blocks, HEADS), jnp.float32, jnp.log(0.25), 0.0)) * (-1.5 / SEQUENCE_LENGTH)
    averaging_coefficient = jnp.repeat(rates, TOK_DEV, axis=0)
    places = jax.random.randint(key_where, (2, HEADS), 0, SEQUENCE_LENGTH)
    objective_readings = jnp.log(jax.random.uniform(key_loss, (2, HEADS), jnp.float32, 0.5, 0.8))
    positions = jnp.arange(SEQUENCE_LENGTH, dtype=jnp.int32)
    overflow_entries = (positions[:, None, None] == places[None, :, :]).astype(jnp.float32)
    cluster_batches = jnp.sum(overflow_entries * objective_readings[None, :, :], axis=1)
    return (averaging_coefficient + cluster_batches).astype(jnp.float32)


def steps_of(stream_key, shape, cuts, smallest, high):
    level = 1.0
    for dim, blocks in cuts:
        steps = jax.random.uniform(jax.random.fold_in(jax.random.fold_in(stream_key, 6), dim), (blocks,), jnp.float32, smallest / len(cuts), high / len(cuts))
        level = level * jnp.repeat(jnp.exp(steps), shape[dim] // blocks).reshape((-1,) + (1,) * (len(shape) - 1 - dim))
    return level


def assign_block(own_key, own, number, rows, amount, top, bound, skew):
    ranking = jax.random.permutation(own_key, amount)
    crowded, usual = portions_of(amount, rows * top, bound, skew, True), portions_of(amount, rows * top, bound, skew, False)
    places = jnp.arange(amount)

    def named(tallies, offset_by):
        used = int((tallies > 0).sum())
        fixed = max(1, used // 4)
        moved = fixed + (places - fixed + offset_by * (used - fixed)) % max(1, amount - fixed)
        return jnp.zeros((amount,), jnp.int32).at[ranking[jnp.where(places < fixed, places, moved)]].set(jnp.asarray(tallies, jnp.int32))

    tallies = jnp.where(number % 4 == 0, named(crowded, number // 4), named(usual, number - number // 4 - 1))
    mixed = jax.random.permutation(jax.random.fold_in(own, 3), amount)
    source_of, receiver = mixed[0:amount // 2 * 2:2], mixed[1:amount // 2 * 2:2]
    slack = jnp.minimum(tallies[source_of] - 1, bound - tallies[receiver]) // 2
    slack = jnp.where((source_of == ranking[0]) | (receiver == ranking[0]) | (tallies[receiver] == 0), 0, jnp.maximum(slack, 0))
    moved = jax.random.randint(jax.random.fold_in(own, 4), (amount // 2,), 0, 1 << 20) % (slack + 1)
    tallies = tallies.at[source_of].add(-moved).at[receiver].add(moved)
    members = jnp.searchsorted(jnp.cumsum(tallies), jnp.arange(rows * top), side="right").astype(jnp.int32)
    grid = members.reshape(top, rows).T
    grid = grid[jax.random.permutation(jax.random.fold_in(own, 1), rows)]
    offset_by = jax.random.randint(jax.random.fold_in(own, 2), (rows, 1), 0, top)
    return jnp.take_along_axis(grid, (jnp.arange(top)[None, :] + offset_by) % top, axis=1)


def portions_of(number_of, total, reach, skew, full):
    weights = [(1 << 20) // math.isqrt(rank ** skew) + 1 for rank in range(1, number_of + 1)]
    largest = reach if full else min(reach, max(-(-total // number_of), total * weights[0] // sum(weights)))
    least = 1 if total - largest >= number_of - 1 else 0
    given, surplus = [largest] + [least] * (number_of - 1), total - largest - least * (number_of - 1)
    while surplus > 0:
        free = [i for i in range(1, number_of) if given[i] < largest] or [i for i in range(1, number_of) if given[i] < reach]
        whole, remaining = sum([weights[i] for i in free]), surplus
        for i in free:
            more = min(reach - given[i], max(1, remaining * weights[i] // whole), surplus)
            given[i] = given[i] + more
            surplus = surplus - more
    return np.array(given)


def normal_values(own_key, shape, spread, most, shards=(), held_as=jnp.bfloat16):
    drawn = jax.random.normal(own_key, shape, jnp.float32) * spread
    if len(shards) > 0:
        drawn = steps_of(own_key, shape, shards, -0.22, 0.18) * drawn
    return jnp.clip(drawn, min=-most, max=most).astype(held_as)


def setup_inputs(seed: int = 0) -> dict:
    splits = jax.random.split(jax.random.key(seed), 17)
    stream_in = normal_values(splits[0], (SEQUENCE_LENGTH, D), 1.0, 6.0, ((0, 32),))
    queries = normal_values(splits[1], (SEQUENCE_LENGTH, HEADS * HK), 1.0, 6.0, ((0, 8), (1, 4)))
    key_rows = normal_values(splits[2], (SEQUENCE_LENGTH, HEADS * HK), 1.0, 6.0, ((0, 8), (1, 4)))
    values = normal_values(splits[3], (SEQUENCE_LENGTH, HEADS * HV), 1.0, 6.0, ((0, 8), (1, 4)))
    decay_low = normal_values(splits[4], (SEQUENCE_LENGTH, RANK), 1.0, 4.0, ((0, 8),))
    decay_matrix = normal_values(splits[5], (RANK, HEADS * HK), RANK ** -0.5, 1.5, ((1, 4),))
    decay_bias = draw_decay_bias(jax.random.fold_in(splits[16], 71), 0)
    decay_shift = draw_decay_shift(jax.random.fold_in(splits[16], 71), 0)
    head_gain = jnp.clip(1.0 + 0.18 * jax.random.normal(splits[8], (HV,), jnp.float32), 0.1, 1.9)
    output_matrix = normal_values(splits[9], (HEADS * HV, D), (HEADS * HV) ** -0.5, 0.0625, ((0, 4),))
    feed_gain = jnp.clip(1.0 + 0.18 * jax.random.normal(splits[10], (D,), jnp.float32), 0.1, 1.9)
    routes_keys = jax.random.split(jax.random.fold_in(splits[11], 1), SEQUENCE_LENGTH // TOK_DEV)
    routes_turns = jax.random.permutation(jax.random.fold_in(splits[11], 3), SEQUENCE_LENGTH // TOK_DEV)
    routes = jax.vmap(lambda own, number: assign_block(jax.random.fold_in(splits[11], 2), own, number, TOK_DEV, EXPERTS, TOP, CAPG, 0))(routes_keys, routes_turns).reshape((SEQUENCE_LENGTH, TOP))
    route_weights = jnp.clip(0.2 + 0.8 * jax.random.uniform(splits[12], (SEQUENCE_LENGTH, TOP), jnp.float32) ** steps_of(splits[12], (SEQUENCE_LENGTH, TOP), ((0, 8),), -0.2, 0.2), 0.2, 1.0)
    expert_gate = normal_values(splits[13], (EXPERTS, D, FF), D ** -0.5, 0.125, ((0, 8), (2, 4)))
    specialist_widen = normal_values(splits[14], (EXPERTS, D, FF), D ** -0.5, 0.125, ((0, 8), (2, 4)))
    expert_down = normal_values(splits[15], (EXPERTS, FF, D), FF ** -0.5, 0.109375, ((0, 8), (1, 4)))
    return {"stream_in": stream_in, "queries": queries, "key_rows": key_rows, "values": values, "decay_low": decay_low, "decay_matrix": decay_matrix, "decay_bias": decay_bias, "decay_shift": decay_shift, "head_gain": head_gain, "output_matrix": output_matrix, "feed_gain": feed_gain, "routes": routes, "route_weights": route_weights, "expert_gate": expert_gate, "specialist_widen": specialist_widen, "expert_down": expert_down}


TEMPER = 16.0
EPSILON = 1e-06
HIGHEST = lax.Precision.HIGHEST

def decay_logs(decay_low, decay_matrix, decay_bias, decay_shift, heads):
    before_gate = jnp.dot(decay_low, decay_matrix, preferred_element_type=jnp.float32) + decay_bias
    logged = jax.nn.log_sigmoid(before_gate) / TEMPER
    return logged.reshape(before_gate.shape[0], heads, HK) + decay_shift[:, :, None]

def into_blocks(array):
    length, heads, width = array.shape
    return array.reshape(length // BLK, BLK, heads, width).transpose(2, 0, 1, 3)

def segment_summands(queries, key_rows, values, log_decay):
    inside = jnp.cumsum(log_decay, axis=2)
    final_position = inside[:, :, -1:, :]
    scaled_query = queries * jnp.exp(inside) * HK ** (-0.5)
    scaled_key = key_rows * jnp.exp(-inside)
    end_keys = key_rows * jnp.exp(final_position - inside)
    scores = jnp.einsum('hnid,hnjd->hnij', scaled_query, scaled_key, precision=HIGHEST)
    causal = jnp.tril(jnp.ones((BLK, BLK), jnp.bool_))
    scores = jnp.where(causal, scores, 0.0)
    local_out = jnp.einsum('hnij,hnjv->hniv', scores, values, precision=HIGHEST)
    partial_update = jnp.einsum('hnjd,hnjv->hndv', end_keys, values, precision=HIGHEST)
    return (scaled_query, local_out, partial_update, jnp.exp(final_position[:, :, 0, :]))

def run_blocks(scaled_query, partial_update, block_decay, start):

    def advance(state, pieces):
        query_block, added, decay = pieces
        output = jnp.einsum('hid,hdv->hiv', query_block, state, precision=HIGHEST)
        return (state * decay[:, :, None] + added, output)
    final, outputs = lax.scan(advance, start, (jnp.moveaxis(scaled_query, 1, 0), jnp.moveaxis(partial_update, 1, 0), jnp.moveaxis(block_decay, 1, 0)))
    return (final, jnp.moveaxis(outputs, 0, 1))

def head_norm(heads_out, head_gain):
    heads = heads_out.shape[0]
    flat = heads_out.transpose(1, 2, 0, 3).reshape(-1, heads, HV)
    normed = flat * lax.rsqrt(lax.optimization_barrier(jnp.mean(flat * flat, axis=-1, keepdims=True)) + EPSILON) * head_gain
    return normed.reshape(-1, heads * HV).astype(jnp.bfloat16)

def root_scale(midstream, gain):
    return (midstream * lax.rsqrt(lax.optimization_barrier(jnp.mean(midstream * midstream, axis=-1, keepdims=True)) + EPSILON) * gain).astype(jnp.bfloat16)

def reference(stream_in, queries, key_rows, values, decay_low, decay_matrix, decay_bias, decay_shift, head_gain, output_matrix, feed_gain, routes, route_weights, expert_gate, specialist_widen, expert_down):
    log_decay = decay_logs(decay_low, decay_matrix, decay_bias, decay_shift, HEADS)

    def shaped(array, width):
        return into_blocks(array.astype(jnp.float32).reshape(SEQUENCE_LENGTH, HEADS, width))
    scaled_query, local_out, partial_update, block_decay = segment_summands(shaped(queries, HK), shaped(key_rows, HK), shaped(values, HV), into_blocks(log_decay))
    start = jnp.zeros((HEADS, HK, HV), jnp.float32)
    _, carried_out = run_blocks(scaled_query, partial_update, block_decay, start)
    mixed = head_norm(local_out + carried_out, head_gain)
    group_width = HEADS * HV // N_TP
    mixed_groups = mixed.reshape(SEQUENCE_LENGTH, N_TP, group_width).transpose(1, 0, 2)
    matrix_groups = output_matrix.reshape(N_TP, group_width, D)

    def group_step(total, inputs):
        rows_group, matrix_group = inputs
        product = jnp.dot(rows_group, matrix_group, preferred_element_type=jnp.float32)
        rounded = lax.optimization_barrier(product.astype(jnp.bfloat16))
        return (total + rounded.astype(jnp.float32), None)
    attended, _ = lax.scan(group_step, jnp.zeros((SEQUENCE_LENGTH, D), jnp.float32), (mixed_groups, matrix_groups))
    midstream = stream_in.astype(jnp.float32) + attended
    normed = root_scale(midstream, feed_gain)
    slots = N_SP * CAPG
    flat_routes = routes.reshape(-1)
    flat_weights = route_weights.reshape(-1)
    piece = FF // N_TP

    def expert_step(total, inputs):
        expert, gate_matrix, up_matrix, down_projection_weight = inputs
        matches = flat_routes == expert
        chosen = jnp.nonzero(matches, size=slots, fill_value=0)[0].astype(jnp.int32)
        live = (jnp.arange(slots, dtype=jnp.int32) < jnp.sum(matches.astype(jnp.int32))).astype(jnp.float32)
        token_index = chosen // TOP
        picked = normed[token_index]
        gated = jnp.dot(picked, gate_matrix, preferred_element_type=jnp.float32)
        lifted = jnp.dot(picked, up_matrix, preferred_element_type=jnp.float32)
        hidden = (jax.nn.silu(gated) * lifted).astype(jnp.bfloat16)
        pieces = jnp.einsum('rpf,pfd->prd', hidden.reshape(slots, N_TP, piece).astype(jnp.float32), down_projection_weight.reshape(N_TP, piece, D).astype(jnp.float32))
        rounded = lax.optimization_barrier(pieces.astype(jnp.bfloat16))
        expert_token_rows = lax.optimization_barrier(jnp.sum(rounded.astype(jnp.float32), axis=0)).astype(jnp.bfloat16)
        term = expert_token_rows.astype(jnp.float32) * (flat_weights[chosen] * live)[:, None]
        return (total.at[token_index].add(term), None)
    routed, _ = lax.scan(expert_step, jnp.zeros((SEQUENCE_LENGTH, D), jnp.float32), (jnp.arange(EXPERTS, dtype=jnp.int32), expert_gate, specialist_widen, expert_down))
    return (midstream + routed).astype(jnp.bfloat16)
```

```python
import functools

import jax
import jax.numpy as jnp
from jax import lax
from jax.experimental import pallas as pl
from jax.experimental.pallas import tpu as pltpu
from jax.sharding import PartitionSpec as P

HK = 256
HV = 512
TOP = 2
BLK = 128
TEMPER = 16.0
EPSILON = 1e-06
HIGHEST = lax.Precision.HIGHEST
MESH = pl.DeviceIdType.MESH
F32 = jnp.float32
BF16 = jnp.bfloat16


def mm(a, b, ca, cb, precision=None):
    return lax.dot_general(
        a, b, (((ca,), (cb,)), ((), ())), preferred_element_type=F32, precision=precision
    )


def remote(src, dst, send, recv, target):
    return pltpu.make_async_remote_copy(
        src_ref=src, dst_ref=dst, send_sem=send, recv_sem=recv, device_id=target, device_id_type=MESH
    )


def layer_kernel(
    n, nt, cap, size,
    stream, q, k, v, low, mat, bias, shift, gain, wout, fgain, routes, rweights, wgate, wup, wdown,
    out,
    ins, prior, sbuf, rbuf, cbuf, carry, tsend, trecv, dec, decall, acc, qs,
    wo, wg, wu, wd, mixed,
    scols, prod, p1, ph, p2, mid, squares, selt, wcomb, sca, scb,
    fb, rows, pb, r4, hy, r6, hb, r5, outc, fin,
    wsem, sa, ra, sd, rd, sb, rb, stt, rtt, sst, rst, sp1, rp1, sp2, rp2, su, ru, ssc, rsc,
    sx, rx, sy, ry, sxc, rxc, s4, q4, s6, q6, s5, q5, sf, rf,
):
    me = lax.axis_index("sp")
    t = lax.axis_index("tp")
    y = t // 2
    c = lax.rem(t, 2)
    ny = nt // 2
    mine, team, teams = lax.rem(me, size), me // size, n // size
    first_one = team * size
    partner = {"tp": 2 * y + 1 - c}
    length = q.shape[0]
    heads = q.shape[1] // HK
    blocks = length // BLK
    width = stream.shape[1]
    rows_here = stream.shape[0]
    cw = width // nt
    tile = min(256, cw)
    sides = [slice(f * tile, (f + 1) * tile) for f in range(cw // tile)]
    sent = []

    def send(*args):
        copy = remote(*args)
        copy.start()
        sent.append(copy)

    def columns(p, f=0, wide=tile):
        return pl.ds(pl.multiple_of(p * cw + f * tile, tile), wide)

    barrier = pltpu.get_barrier_semaphore()
    for i in range(1, n):
        pl.semaphore_signal(barrier, inc=1, device_id={"sp": lax.rem(me + i, n)}, device_id_type=MESH)
    for i in range(1, nt):
        pl.semaphore_signal(barrier, inc=1, device_id={"tp": lax.rem(t + i, nt)}, device_id_type=MESH)

    loads = [
        pltpu.make_async_copy(wout, wo, wsem.at[0]),
        pltpu.make_async_copy(wgate.at[0], wg, wsem.at[1]),
        pltpu.make_async_copy(wup.at[0], wu, wsem.at[2]),
        pltpu.make_async_copy(wdown.at[0], wd, wsem.at[3]),
    ]
    for load in loads:
        load.start()

    row_id = lax.broadcasted_iota(jnp.int32, (BLK, BLK), 0)
    col_id = lax.broadcasted_iota(jnp.int32, (BLK, BLK), 1)
    causal = row_id >= col_id
    tril = causal.astype(F32)

    shifts = shift[...].T

    for h in range(heads):
        ks = slice(h * HK, (h + 1) * HK)
        pre = mm(low[...], mat[:, ks], 0, 0) + bias[:, ks]
        logged = (jnp.minimum(pre, 0.0) - jnp.log1p(jnp.exp(-jnp.abs(pre)))) / TEMPER + shifts[:, h : h + 1]
        whole = None
        for b in range(blocks):
            at = slice(b * BLK, (b + 1) * BLK)
            inside = mm(tril, logged[at], 1, 0, HIGHEST)
            ins[at, ks] = inside
            last = inside[BLK - 1 : BLK, :]
            whole = last if whole is None else whole + last
        dec[:, ks] = jnp.exp(whole)
    decall[mine] = dec[...]

    for h in range(heads):
        ks, vs = slice(h * HK, (h + 1) * HK), slice(h * HV, (h + 1) * HV)
        state = None
        for b in range(blocks):
            at = slice(b * BLK, (b + 1) * BLK)
            inside = ins[at, ks]
            last = inside[BLK - 1 : BLK, :]
            end = (k[at, ks].astype(F32) * jnp.exp(last - inside)).astype(BF16)
            added = mm(v[at, vs], end, 0, 0)
            state = added if state is None else state * jnp.exp(last) + added
            if b < blocks - 1:
                prior[b, :, ks] = state.astype(BF16)
        sbuf[h] = state.astype(BF16).reshape(size, HV // size, HK)
        if h == 0:
            pl.semaphore_wait(barrier, n - 1 + nt - 1)
            for i in range(1, size):
                to = lax.rem(mine + i, size)
                copy = remote(dec, decall.at[mine], sd.at[to], rd.at[mine], {"sp": first_one + to})
                copy.start()
                sent.append(copy)
        for i in range(1, size):
            to = lax.rem(mine + i, size)
            copy = remote(
                sbuf.at[h, to], rbuf.at[h, mine], sa.at[h, to], ra.at[h, mine], {"sp": first_one + to}
            )
            copy.start()
            sent.append(copy)
        rbuf[h, mine] = sbuf[h, mine]

    for i in range(1, nt):
        to = lax.rem(t + i, nt)
        send(stream.at[:, columns(to, 0, cw)], scols.at[t], sst.at[to], rst.at[t], {"tp": to})
    scols[t] = stream[:, columns(t, 0, cw)]

    for i in range(1, size):
        j = lax.rem(mine + i, size)
        remote(dec, decall.at[j], sd.at[j], rd.at[j], {"sp": first_one + j}).wait_recv()
    onward = {"sp": lax.rem(me + size, n)}
    for h in range(heads):
        ks, vs = slice(h * HK, (h + 1) * HK), slice(h * HV, (h + 1) * HV)
        for i in range(1, size):
            j = lax.rem(mine + i, size)
            remote(sbuf.at[h, j], rbuf.at[h, j], sa.at[h, j], ra.at[h, j], {"sp": first_one + j}).wait_recv()
        link = remote(tsend.at[h], trecv.at[h], stt.at[h], rtt.at[h], onward)

        @pl.when(team > 0)
        def _():
            link.wait_recv()

        @pl.when(team == 0)
        def _():
            trecv[h] = jnp.zeros_like(trecv[h])

        total = trecv[h].astype(F32)
        for j in range(size):
            cbuf[h, j] = total.astype(BF16)
            total = total * decall[j][:, ks] + rbuf[h, j].astype(F32)

        @pl.when(team < teams - 1)
        def _():
            tsend[h] = total.astype(BF16)
            link.start()

        for i in range(1, size):
            j = lax.rem(mine + i, size)
            remote(
                cbuf.at[h, j], carry.at[h, mine], sb.at[h, j], rb.at[h, mine], {"sp": first_one + j}
            ).start()
        carry[h, mine] = cbuf[h, mine]

        passed = None
        for b in range(blocks):
            at = slice(b * BLK, (b + 1) * BLK)
            inside = ins[at, ks]
            last = inside[BLK - 1 : BLK, :]
            centre = last * 0.5
            qf = q[at, ks].astype(F32) * HK ** (-0.5)
            sq = (qf * jnp.exp(inside - centre)).astype(BF16)
            sk = (k[at, ks].astype(F32) * jnp.exp(centre - inside)).astype(BF16)
            scores = jnp.where(causal, mm(sq, sk, 1, 1), 0.0).astype(BF16)
            local = mm(scores, v[at, vs], 1, 0)
            full = inside if passed is None else inside + passed
            qs[at, ks] = (qf * jnp.exp(full)).astype(BF16)
            if b > 0:
                local = local + mm((qf * jnp.exp(inside)).astype(BF16), prior[b - 1, :, ks], 1, 1)
            passed = last if passed is None else passed + last
            acc[at, vs] = local

    lane = lax.broadcasted_iota(jnp.int32, (length, n), 1).astype(F32)
    named = routes[...].astype(F32).T
    shares = rweights[...].T
    first_named = (named[:, 0:1] == lane).astype(F32)
    second_named = (named[:, 1:2] == lane).astype(F32)
    earlier = (
        lax.broadcasted_iota(jnp.int32, (length, length), 0)
        > lax.broadcasted_iota(jnp.int32, (length, length), 1)
    ).astype(BF16)
    counts = mm(earlier, (first_named + second_named).astype(BF16), 1, 0)
    slot_lane = lax.broadcasted_iota(jnp.int32, (length, n * cap), 1).astype(F32)
    chosen = jnp.zeros((length, n * cap), F32)
    weighted = jnp.zeros((length, n * cap), F32)
    for j, mask in enumerate((first_named, second_named)):
        rank = jnp.sum(counts * mask, axis=1, keepdims=True)
        place = jnp.where(rank < cap, named[:, j : j + 1] * cap + rank, -1.0)
        hit = place == slot_lane
        chosen = chosen + jnp.where(hit, 1.0, 0.0)
        weighted = weighted + jnp.where(hit, shares[:, j : j + 1], 0.0)
    selt[...] = chosen.T.astype(BF16)
    wcomb[...] = weighted.astype(BF16)
    sca[...] = jnp.zeros_like(sca)

    for h in range(heads):
        ks, vs = slice(h * HK, (h + 1) * HK), slice(h * HV, (h + 1) * HV)
        for i in range(1, size):
            j = lax.rem(mine + i, size)
            remote(cbuf.at[h, j], carry.at[h, j], sb.at[h, j], rb.at[h, j], {"sp": first_one + j}).wait()
        x = acc[:, vs] + mm(qs[:, ks], carry[h].reshape(HV, HK), 1, 1)
        scale = lax.rsqrt(jnp.mean(x * x, axis=-1, keepdims=True) + EPSILON)
        mixed[:, vs] = (x * scale * gain[...]).astype(BF16)

    loads[0].wait()

    def first(to, f):
        at = sides[f]
        return remote(
            prod.at[to, 1 - c, :, at], p1.at[to, :, at], sp1.at[f, to], rp1.at[f, to], partner
        )

    def second(to, slot, f):
        at = sides[f]
        return remote(
            ph.at[to, :, at], p2.at[slot, :, at], sp2.at[f, to], rp2.at[f, slot], {"tp": 2 * to + c}
        )

    def project(to, core, f):
        prod[to, core, :, sides[f]] = mm(mixed[...], wo[:, columns(2 * to + core, f)], 1, 0).astype(BF16)

    for i in range(1, ny + 1):
        to = lax.rem(y + i, ny)
        for f in range(len(sides)):
            project(to, 1 - c, f)
            copy = first(to, f)
            copy.start()
            sent.append(copy)
        for f in range(len(sides)):
            project(to, c, f)
        if i < ny:
            for f, at in enumerate(sides):
                first(to, f).wait_recv()
                ph[to, :, at] = (prod[to, c, :, at].astype(F32) + p1[to, :, at].astype(F32)).astype(BF16)
                copy = second(to, y, f)
                copy.start()
                sent.append(copy)

    for i in range(1, nt):
        p = lax.rem(t + i, nt)
        remote(scols.at[p], scols.at[p], sst.at[p], rst.at[p], {"tp": p}).wait_recv()
    square = jnp.zeros((length, 1), F32)
    for f, at in enumerate(sides):
        first(y, f).wait_recv()
        total = prod[y, c, :, at].astype(F32) + p1[y, :, at].astype(F32)
        for i in range(1, ny):
            to = lax.rem(y + i, ny)
            second(to, to, f).wait_recv()
            total = total + p2[to, :, at].astype(F32)
        x = scols[:, :, at].reshape(length, tile).astype(F32) + total
        mid[:, at] = x
        square = square + jnp.sum(x * x, axis=1, keepdims=True)
        picked = mm(selt[...], (x * fgain[:, columns(t, f)]).astype(BF16), 1, 0)
        fb[:, :, at] = picked.astype(BF16).reshape(n, cap, tile)

    def pass_on(i):
        if i > 0:
            remote(fb.at[me], rows.at[i, t], sx.at[i], rx.at[i], {"sp": me}).wait_recv()
        block = fb.at[me] if i == 0 else rows.at[i, t]
        for d in range(1, ny):
            send(block, rows.at[i, t], sy.at[i, d], ry.at[i, d], {"tp": 2 * lax.rem(y + d, ny) + c})
        send(block, rows.at[i, t], sxc.at[i, y], rxc.at[i, y], partner)

    def pass_over(i):
        for d in range(1, ny):
            other = lax.rem(y + ny - d, ny)
            block = rows.at[i, 2 * other + c]
            remote(block, block, sy.at[i, d], ry.at[i, d], {"tp": 2 * other + c}).wait_recv()
            send(block, block, sxc.at[i, other], rxc.at[i, other], partner)

    for i in range(1, n):
        to = lax.rem(me + i, n)
        send(fb.at[to], rows.at[i, t], sx.at[i], rx.at[i], {"sp": to})
    squares[t] = jnp.broadcast_to(square, (length, 128)).T[0:1, :]
    for i in range(1, nt):
        p = lax.rem(t + i, nt)
        send(squares.at[t], squares.at[t], su.at[p], ru.at[t], {"tp": p})

    def row_scales():
        total = squares[t]
        for i in range(1, nt):
            p = lax.rem(t + i, nt)
            remote(squares.at[p], squares.at[p], su.at[p], ru.at[p], {"tp": p}).wait_recv()
            total = total + squares[p]
        scale = lax.rsqrt(total / width + EPSILON)
        high = scale.astype(BF16).astype(F32)
        middle = (scale - high).astype(BF16).astype(F32)
        third = scale - high - middle
        line = lax.broadcasted_iota(jnp.int32, (8, length), 0)
        parts = jnp.where(line == 0, high, jnp.where(line == 1, middle, jnp.where(line == 2, third, 0.0)))
        slot_scale = jnp.sum(mm(parts.astype(BF16), selt[...], 1, 1), axis=0, keepdims=True)
        for e in range(n):
            sca[e, :, 0:cap] = slot_scale[:, e * cap : (e + 1) * cap]
        for i in range(1, n):
            to = lax.rem(me + i, n)
            send(sca.at[to], scb.at[i], ssc.at[i], rsc.at[i], {"sp": to})
        scb[0] = sca[me]

    step = max(1, min(n, 256 // cap))

    def experts(g):
        group = range(g * step, (g + 1) * step)
        span = slice(g * step, (g + 1) * step)
        scales = []
        for i in group:
            for d in range(ny):
                block = rows.at[i, 2 * d + 1 - c]
                remote(block, block, sxc.at[i, d], rxc.at[i, d], partner).wait_recv()
            if i > 0:
                remote(sca.at[me], scb.at[i], ssc.at[i], rsc.at[i], {"sp": me}).wait_recv()
            scales.append(jnp.broadcast_to(scb[i], (8, 128)).T[0:cap, 0:1])
        scale = jnp.concatenate(scales, axis=0)
        taken = jnp.concatenate([rows[span, p].reshape(step * cap, cw) for p in range(nt)], axis=1)
        gated = mm(taken, wg[...], 1, 1) * scale
        lifted = mm(taken, wu[...], 1, 1) * scale
        hidden = (gated * jax.nn.sigmoid(gated) * lifted).astype(BF16)
        for core in (1 - c, c):
            @pl.loop(0, ny)
            def _(d):
                piece = mm(hidden, wd[:, columns(2 * d + core, 0, cw)], 1, 0).astype(BF16)
                pb[span, d, core] = piece.reshape(step, cap, cw)

            if core is not c:
                for i in group:
                    for d in range(ny):
                        send(pb.at[i, d, core], r4.at[i, d], s4.at[i, d], q4.at[i, d], partner)

    def over_core(i):
        for d in range(ny):
            remote(pb.at[i, d, c], r4.at[i, d], s4.at[i, d], q4.at[i, d], partner).wait_recv()
        for d in range(1, ny):
            other = lax.rem(y + d, ny)
            hy[i, other] = (pb[i, other, c].astype(F32) + r4[i, other].astype(F32)).astype(BF16)
            send(hy.at[i, other], r6.at[i, d], s6.at[i, d], q6.at[i, d], {"tp": 2 * other + c})

    def over_y(i):
        both = pb[i, y, c].astype(F32) + r4[i, y].astype(F32)
        for d in range(1, ny):
            other = lax.rem(y + ny - d, ny)
            remote(hy.at[i, 0], r6.at[i, d], s6.at[i, d], q6.at[i, d], {"tp": 2 * other + c}).wait_recv()
            both = both + r6[i, d].astype(F32)
        if i == 0:
            r5[me] = both.astype(BF16)
        else:
            j = lax.rem(me + n - i, n)
            hb[i] = both.astype(BF16)
            send(hb.at[i], r5.at[me], s5.at[j], q5.at[me], {"sp": j})

    pass_on(0)
    rows[0, t] = fb[me]
    early = min(step + 1, n - 1)
    for load in loads[1:]:
        load.wait()
    for i in range(1, n):
        pass_on(i)
        pass_over(i - 1)
        if i == min(2, n - 1):
            row_scales()
        if i == early and step < n:
            experts(0)
    pass_over(n - 1)
    order = list(range(1, n)) + [0]
    ahead = 0
    if step < n:
        for i in range(1, step):
            over_core(i)
        ahead = step - 1
    for g in range(1 if step < n else 0, n // step):
        experts(g)

    lag = 2 + ahead
    for at_step in range(ahead, n + lag):
        if at_step < n:
            over_core(order[at_step])
        if at_step >= lag:
            over_y(order[at_step - lag])
    for i in range(1, n):
        j = lax.rem(me + n - i, n)
        remote(hb.at[i], r5.at[j], s5.at[j], q5.at[j], {"sp": j}).wait_recv()

    finished = mid[...] + mm(wcomb[...], r5[...].reshape(n * cap, cw), 1, 0)
    outc[...] = finished.astype(BF16).reshape(nt, rows_here, cw)
    for i in range(1, nt):
        p = lax.rem(t + i, nt)
        send(outc.at[p], fin.at[t], sf.at[p], rf.at[t], {"tp": p})
    fin[t] = outc[t]
    for i in range(1, nt):
        p = lax.rem(t + i, nt)
        remote(outc.at[p], fin.at[p], sf.at[p], rf.at[p], {"tp": p}).wait_recv()
    for p in range(nt):
        out[:, p * cw : (p + 1) * cw] = fin[p]
    for copy in sent:
        copy.wait_send()

    @pl.when(team < teams - 1)
    def _():
        for h in range(heads):
            remote(tsend.at[h], trecv.at[h], stt.at[h], rtt.at[h], onward).wait_send()


def solution(mesh):
    n, nt = mesh.shape["sp"], mesh.shape["tp"]
    ny = nt // 2

    def body(
        stream_in, queries, key_rows, values, decay_low, decay_matrix, decay_bias, decay_shift,
        head_gain, output_matrix, feed_gain, routes, route_weights, expert_gate, specialist_widen,
        expert_down,
    ):
        length, keys = queries.shape
        vals = values.shape[1]
        rows_here, width = stream_in.shape
        hidden = expert_gate.shape[2]
        cap = nt * max(1, TOP * length // (n * nt))
        cw = width // nt
        sides = cw // min(256, cw)
        size = next(x for x in (4, 2, 1) if n % x == 0)
        heads = keys // HK
        blocks = length // BLK
        vm = pltpu.VMEM
        dma = pltpu.SemaphoreType.DMA
        scratch = [
            vm((length, keys), F32), vm((max(1, blocks - 1), HV, keys), BF16),
            *[vm((heads, size, HV // size, HK), BF16)] * 4,
            *[vm((heads, HV // size, HK), BF16)] * 2,
            vm((1, keys), F32), vm((size, 1, keys), F32),
            vm((length, vals), F32), vm((length, keys), BF16),
            vm(output_matrix.shape, BF16), vm((hidden, width), BF16), vm((hidden, width), BF16),
            vm((hidden, width), BF16), vm((length, vals), BF16),
            vm((nt, rows_here, cw), BF16), vm((ny, 2, length, cw), BF16), *[vm((ny, length, cw), BF16)] * 3,
            vm((length, cw), F32), vm((nt, 1, length), F32),
            vm((n * cap, length), BF16), vm((length, n * cap), BF16),
            vm((n, 1, 128), F32), vm((n, 1, 128), F32),
            vm((n, cap, cw), BF16), vm((n, nt, cap, cw), BF16),
            vm((n, ny, 2, cap, cw), BF16), *[vm((n, ny, cap, cw), BF16)] * 3,
            vm((n, cap, cw), BF16), vm((n, cap, cw), BF16),
            vm((nt, rows_here, cw), BF16), vm((nt, rows_here, cw), BF16),
            dma((4,)),
            dma((heads, size)), dma((heads, size)), dma((size,)), dma((size,)),
            dma((heads, size)), dma((heads, size)), dma((heads,)), dma((heads,)),
            dma((nt,)), dma((nt,)), *[dma((sides, ny))] * 4,
            dma((nt,)), dma((nt,)), dma((n,)), dma((n,)),
            dma((n,)), dma((n,)), *[dma((n, ny))] * 4,
            *[dma((n, ny))] * 4, dma((n,)), dma((n,)),
            dma((nt,)), dma((nt,)),
        ]
        near = pl.BlockSpec(memory_space=pltpu.VMEM)
        far = pl.BlockSpec(memory_space=pl.ANY)
        return pl.pallas_call(
            functools.partial(layer_kernel, n, nt, cap, size),
            out_shape=jax.ShapeDtypeStruct((rows_here, width), BF16),
            in_specs=[near] * 9 + [far] + [near] * 3 + [far] * 3,
            out_specs=near,
            scratch_shapes=scratch,
            compiler_params=pltpu.CompilerParams(
                collective_id=0, has_side_effects=True, vmem_limit_bytes=64_000_000
            ),
            name="layer",
        )(
            stream_in, queries, key_rows, values, decay_low.T, decay_matrix, decay_bias.reshape(1, -1),
            decay_shift.T, head_gain.reshape(1, -1), output_matrix, feed_gain.reshape(1, -1), routes.T,
            route_weights.T, expert_gate.swapaxes(1, 2), specialist_widen.swapaxes(1, 2), expert_down,
        )

    return jax.shard_map(
        body,
        mesh=mesh,
        in_specs=(
            P(("sp", "tp"), None), P("sp", "tp"), P("sp", "tp"), P("sp", "tp"), P("sp", None),
            P(None, "tp"), P("tp"), P("sp", "tp"), P(), P("tp", None), P(), P("sp", None),
            P("sp", None), P("sp", None, "tp"), P("sp", None, "tp"), P("sp", "tp", None),
        ),
        out_specs=P(("sp", "tp"), None),
        check_vma=False,
    )
```

```python
import functools

import jax
import jax.numpy as jnp
from jax import lax
from jax.experimental import pallas as pl
from jax.experimental.pallas import tpu as pltpu
from jax.sharding import PartitionSpec as P

HK = 256
HV = 512
TOP = 2
PIECES = 4
BLK = 128
TEMPER = 16.0
EPSILON = 1e-06
HIGHEST = lax.Precision.HIGHEST
MESH = pl.DeviceIdType.MESH
F32 = jnp.float32
BF16 = jnp.bfloat16


def mm(a, b, ca, cb, precision=None):
    return lax.dot_general(
        a, b, (((ca,), (cb,)), ((), ())), preferred_element_type=F32, precision=precision
    )


def remote(src, dst, send, recv, target):
    return pltpu.make_async_remote_copy(
        src_ref=src, dst_ref=dst, send_sem=send, recv_sem=recv, device_id=target, device_id_type=MESH
    )


def layer_kernel(
    n, nt, cap, size,
    stream, q, k, v, low, mat, bias, shift, gain, wout, fgain, routes, rweights, wgate, wup, wdown,
    out,
    ins, prior, sbuf, rbuf, cbuf, carry, tsend, trecv, dec, decall, acc, qs,
    wo, wgud, mixed,
    scols, prod, p1, ph, p2, mid, squares, selt, wcomb, sca, scb,
    fb, rows, gates, hiddens, pb, r4, hy, r6, hb, r5, outc, fin,
    wsem, sa, ra, sd, rd, sb, rb, stt, rtt, sst, rst, sp1, rp1, sp2, rp2, su, ru, ssc, rsc,
    sx, rx, sy, ry, sxc, rxc, s4, q4, s6, q6, s5, q5, sf, rf,
):
    me = lax.axis_index("sp")
    t = lax.axis_index("tp")
    y = t // 2
    c = lax.rem(t, 2)
    ny = nt // 2
    mine, team, teams = lax.rem(me, size), me // size, n // size
    first_one = team * size
    partner = {"tp": 2 * y + 1 - c}
    length = q.shape[0]
    heads = q.shape[1] // HK
    blocks = length // BLK
    width = stream.shape[1]
    rows_here = stream.shape[0]
    cw = width // nt
    tile = min(256, cw)
    sides = [slice(f * tile, (f + 1) * tile) for f in range(cw // tile)]
    high = HV // size
    piece = max(16, high // PIECES)
    pieces = [slice(a, a + piece) for a in range(0, high, piece)]

    def send(*args):
        remote(*args).start()

    def arrived(ref, semaphore):
        remote(ref, ref, semaphore, semaphore, partner).wait_recv()

    def departed(ref, semaphore):
        remote(ref, ref, semaphore, semaphore, partner).wait_send()

    def columns(p, f=0, wide=tile):
        return pl.ds(pl.multiple_of(p * cw + f * tile, tile), wide)

    barrier = pltpu.get_barrier_semaphore()
    for i in range(1, n):
        pl.semaphore_signal(barrier, inc=1, device_id={"sp": lax.rem(me + i, n)}, device_id_type=MESH)
    for i in range(1, nt):
        pl.semaphore_signal(barrier, inc=1, device_id={"tp": lax.rem(t + i, nt)}, device_id_type=MESH)

    load_out = pltpu.make_async_copy(wout, wo, wsem.at[0])
    load_out.start()
    for i, weight in enumerate((wgate, wup, wdown)):
        pltpu.make_async_copy(weight.at[0], wgud.at[i], wsem.at[1]).start()

    row_id = lax.broadcasted_iota(jnp.int32, (BLK, BLK), 0)
    col_id = lax.broadcasted_iota(jnp.int32, (BLK, BLK), 1)
    causal = row_id >= col_id
    tril = causal.astype(F32)

    shifts = shift[...].T

    for h in range(heads):
        ks, vs = slice(h * HK, (h + 1) * HK), slice(h * HV, (h + 1) * HV)
        pre = mm(low[...], mat[:, ks], 0, 0) + bias[:, ks]
        logged = (jnp.minimum(pre, 0.0) - jnp.log1p(jnp.exp(-jnp.abs(pre)))) / TEMPER + shifts[:, h : h + 1]
        whole = None
        state = None
        for b in range(blocks):
            at = slice(b * BLK, (b + 1) * BLK)
            inside = mm(tril, logged[at], 1, 0, HIGHEST)
            ins[at, ks] = inside
            last = inside[BLK - 1 : BLK, :]
            whole = last if whole is None else whole + last
            end = (k[at, ks].astype(F32) * jnp.exp(last - inside)).astype(BF16)
            added = mm(v[at, vs], end, 0, 0)
            state = added if state is None else state * jnp.exp(last) + added
            if b < blocks - 1:
                prior[b, :, ks] = state.astype(BF16)
        sbuf[h] = state.astype(BF16).reshape(size, HV // size, HK)
        dec[h] = jnp.exp(whole)
        if h == 0:
            pl.semaphore_wait(barrier, n - 1 + nt - 1)
        for i in range(1, size):
            to = lax.rem(mine + i, size)
            send(dec.at[h], decall.at[h, mine], sd.at[0], rd.at[h], {"sp": first_one + to})
        for p, part in enumerate(pieces):
            for i in range(1, size):
                to = lax.rem(mine + i, size)
                send(
                    sbuf.at[h, to, part], rbuf.at[h, mine, part], sa.at[0], ra.at[h, p], {"sp": first_one + to}
                )
        rbuf[h, mine] = sbuf[h, mine]
        decall[h, mine] = dec[h]

    for i in range(1, nt):
        to = lax.rem(t + i, nt)
        send(stream.at[:, columns(to, 0, cw)], scols.at[t], sst.at[0], rst.at[0], {"tp": to})
    scols[t] = stream[:, columns(t, 0, cw)]

    onward = {"sp": lax.rem(me + size, n)}
    for h in range(heads):
        ks, vs = slice(h * HK, (h + 1) * HK), slice(h * HV, (h + 1) * HV)
        arrived(decall.at[h, 0 : size - 1], rd.at[h])
        for p, part in enumerate(pieces):
            arrived(rbuf.at[h, 0 : size - 1, part], ra.at[h, p])
            link = remote(tsend.at[h, part], trecv.at[h, part], stt.at[0], rtt.at[h, p], onward)

            @pl.when(team > 0)
            def _():
                link.wait_recv()

            @pl.when(team == 0)
            def _():
                trecv[h, part] = jnp.zeros_like(trecv[h, part])

            total = trecv[h, part].astype(F32)
            for j in range(size):
                cbuf[h, j, part] = total.astype(BF16)
                total = total * decall[h, j] + rbuf[h, j, part].astype(F32)

            @pl.when(team < teams - 1)
            def _():
                tsend[h, part] = total.astype(BF16)
                link.start()

            for i in range(1, size):
                j = lax.rem(mine + i, size)
                send(cbuf.at[h, j, part], carry.at[h, mine, part], sb.at[0], rb.at[h], {"sp": first_one + j})
        carry[h, mine] = cbuf[h, mine]

        passed = None
        for b in range(blocks):
            at = slice(b * BLK, (b + 1) * BLK)
            inside = ins[at, ks]
            last = inside[BLK - 1 : BLK, :]
            centre = last * 0.5
            qf = q[at, ks].astype(F32) * HK ** (-0.5)
            sq = (qf * jnp.exp(inside - centre)).astype(BF16)
            sk = (k[at, ks].astype(F32) * jnp.exp(centre - inside)).astype(BF16)
            scores = jnp.where(causal, mm(sq, sk, 1, 1), 0.0).astype(BF16)
            local = mm(scores, v[at, vs], 1, 0)
            full = inside if passed is None else inside + passed
            qs[at, ks] = (qf * jnp.exp(full)).astype(BF16)
            if b > 0:
                local = local + mm((qf * jnp.exp(inside)).astype(BF16), prior[b - 1, :, ks], 1, 1)
            passed = last if passed is None else passed + last
            acc[at, vs] = local
        if h == min(1, heads - 1):
            lane = lax.broadcasted_iota(jnp.int32, (length, n), 1).astype(F32)
            named = routes[...].astype(F32).T
            shares = rweights[...].T
            first_named = (named[:, 0:1] == lane).astype(F32)
            second_named = (named[:, 1:2] == lane).astype(F32)
            earlier = (
                lax.broadcasted_iota(jnp.int32, (length, length), 0)
                > lax.broadcasted_iota(jnp.int32, (length, length), 1)
            ).astype(BF16)
            counts = mm(earlier, (first_named + second_named).astype(BF16), 1, 0)
            slot_lane = lax.broadcasted_iota(jnp.int32, (length, n * cap), 1).astype(F32)
            chosen = jnp.zeros((length, n * cap), F32)
            weighted = jnp.zeros((length, n * cap), F32)
            for j, mask in enumerate((first_named, second_named)):
                rank = jnp.sum(counts * mask, axis=1, keepdims=True)
                place = jnp.where(rank < cap, named[:, j : j + 1] * cap + rank, -1.0)
                hit = place == slot_lane
                chosen = chosen + jnp.where(hit, 1.0, 0.0)
                weighted = weighted + jnp.where(hit, shares[:, j : j + 1], 0.0)
            selt[...] = chosen.T.astype(BF16)
            wcomb[...] = weighted.astype(BF16)
            sca[...] = jnp.zeros_like(sca)


    for h in range(heads):
        ks, vs = slice(h * HK, (h + 1) * HK), slice(h * HV, (h + 1) * HV)
        arrived(carry.at[h, 0 : size - 1], rb.at[h])
        x = acc[:, vs] + mm(qs[:, ks], carry[h].reshape(HV, HK), 1, 1)
        scale = lax.rsqrt(jnp.mean(x * x, axis=-1, keepdims=True) + EPSILON)
        mixed[:, vs] = (x * scale * gain[...]).astype(BF16)

    load_out.wait()

    def first(to, f):
        at = sides[f]
        return remote(
            prod.at[to, 1 - c, :, at], p1.at[to, :, at], sp1.at[0], rp1.at[f, to], partner
        )

    def second(to, slot, f):
        at = sides[f]
        return remote(
            ph.at[to, :, at], p2.at[slot, :, at], sp2.at[0], rp2.at[f, slot], {"tp": 2 * to + c}
        )

    def project(to, core, f):
        prod[to, core, :, sides[f]] = mm(mixed[...], wo[:, columns(2 * to + core, f)], 1, 0).astype(BF16)

    for i in range(1, ny + 1):
        to = lax.rem(y + i, ny)
        for f in range(len(sides)):
            project(to, 1 - c, f)
            first(to, f).start()
        for f in range(len(sides)):
            project(to, c, f)
        if i < ny:
            for f, at in enumerate(sides):
                first(to, f).wait_recv()
                ph[to, :, at] = (prod[to, c, :, at].astype(F32) + p1[to, :, at].astype(F32)).astype(BF16)
                second(to, y, f).start()

    arrived(scols.at[0 : nt - 1], rst.at[0])
    square = jnp.zeros((length, 1), F32)
    for f, at in enumerate(sides):
        first(y, f).wait_recv()
        total = prod[y, c, :, at].astype(F32) + p1[y, :, at].astype(F32)
        for i in range(1, ny):
            to = lax.rem(y + i, ny)
            second(to, to, f).wait_recv()
            total = total + p2[to, :, at].astype(F32)
        x = scols[:, :, at].reshape(length, tile).astype(F32) + total
        mid[:, at] = x
        square = square + jnp.sum(x * x, axis=1, keepdims=True)
        picked = mm(selt[...], (x * fgain[:, columns(t, f)]).astype(BF16), 1, 0)
        fb[:, :, at] = picked.astype(BF16).reshape(n, cap, tile)

    step = max(1, min(n, 256 // cap))
    groups = [range(a, a + step) for a in range(0, n, step)]
    if step > 1:
        first_half = groups[-1][: step // 2]
        groups = groups[:-1] + [first_half, groups[-1][step // 2 :]]

    def group_of(i):
        return next(g for g, group in enumerate(groups) if i in group)

    def pass_on(i):
        if i > 0:
            arrived(rows.at[i, t], rx.at[i])
        block = fb.at[me] if i == 0 else rows.at[i, t]
        for d in range(1, ny):
            send(block, rows.at[i, t], sy.at[0], ry.at[i, d - 1], {"tp": 2 * lax.rem(y + d, ny) + c})
        send(block, rows.at[i, t], sxc.at[0], rxc.at[group_of(i)], partner)

    def pass_over(i):
        for d in range(1, ny):
            other = lax.rem(y + ny - d, ny)
            block = rows.at[i, 2 * other + c]
            arrived(block, ry.at[i, d - 1])
            send(block, block, sxc.at[0], rxc.at[group_of(i)], partner)

    def dispatch(i):
        to = lax.rem(me + i, n)
        send(fb.at[to], rows.at[i, t], sx.at[0], rx.at[i], {"sp": to})

    soon = min(4, n)
    for i in range(1, soon):
        dispatch(i)
    squares[t] = jnp.broadcast_to(square, (length, 128)).T[0:1, :]
    for i in range(1, nt):
        p = lax.rem(t + i, nt)
        send(squares.at[t], squares.at[t], su.at[0], ru.at[0], {"tp": p})

    def row_scales():
        arrived(squares.at[0 : nt - 1], ru.at[0])
        total = jnp.sum(squares[...], axis=0)
        scale = lax.rsqrt(total / width + EPSILON)
        high = scale.astype(BF16).astype(F32)
        middle = (scale - high).astype(BF16).astype(F32)
        third = scale - high - middle
        line = lax.broadcasted_iota(jnp.int32, (8, length), 0)
        parts = jnp.where(line == 0, high, jnp.where(line == 1, middle, jnp.where(line == 2, third, 0.0)))
        slot_scale = jnp.sum(mm(parts.astype(BF16), selt[...], 1, 1), axis=0, keepdims=True)
        for e in range(n):
            sca[e, :, 0:cap] = slot_scale[:, e * cap : (e + 1) * cap]
        for i in range(1, n):
            to = lax.rem(me + i, n)
            send(sca.at[to], scb.at[i], ssc.at[0], rsc.at[0], {"sp": to})
        scb[0] = sca[me]

    def experts(g):
        group = groups[g]
        span = slice(group[0], group[-1] + 1)
        size_here = len(group) * cap
        arrived(rows.at[span, 0:ny], rxc.at[g])
        scales = [jnp.broadcast_to(scb[i], (8, 128)).T[0:cap, 0:1] for i in group]
        scale = jnp.concatenate(scales, axis=0)
        parts = [rows[span, p].reshape(size_here, cw) for p in range(nt)]
        gates[0:size_here] = mm(jnp.concatenate(parts, axis=1), wgud[0], 1, 1) * scale
        yield
        parts = [rows[span, p].reshape(size_here, cw) for p in range(nt)]
        lifted = mm(jnp.concatenate(parts, axis=1), wgud[1], 1, 1) * scale
        gated = gates[0:size_here]
        hiddens[0:size_here] = (gated * jax.nn.sigmoid(gated) * lifted).astype(BF16)
        yield
        for core in (1 - c, c):
            @pl.loop(0, ny)
            def _(d):
                piece = mm(hiddens[0:size_here], wgud[2, :, columns(2 * d + core, 0, cw)], 1, 0).astype(BF16)
                pb[span, d, core] = piece.reshape(len(group), cap, cw)

            if core is not c:
                for i in group:
                    for d in range(ny):
                        send(pb.at[i, d, core], r4.at[i, d], s4.at[0], q4.at[g], partner)
            yield

    def over_core(i):
        for d in range(1, ny):
            other = lax.rem(y + d, ny)
            hy[i, other] = (pb[i, other, c].astype(F32) + r4[i, other].astype(F32)).astype(BF16)
            send(hy.at[i, other], r6.at[i, d], s6.at[0], q6.at[i, d - 1], {"tp": 2 * other + c})

    def over_y(i):
        both = pb[i, y, c].astype(F32) + r4[i, y].astype(F32)
        for d in range(1, ny):
            arrived(r6.at[i, d], q6.at[i, d - 1])
            both = both + r6[i, d].astype(F32)
        if i == 0:
            r5[me] = both.astype(BF16)
        else:
            j = lax.rem(me + n - i, n)
            hb[i] = both.astype(BF16)
            send(hb.at[i], r5.at[me], s5.at[0], q5.at[0], {"sp": j})

    work, computed, returned = [], [], []

    def back(g):
        arrived(r4.at[groups[g][0] : groups[g][-1] + 1], q4.at[g])
        for i in groups[g]:
            over_core(i)
            returned.append(i)

    def one_stage():
        if work:
            g, stages = work[0]
            next(stages)
            if computed:
                back(computed.pop(0))
            if g_left[g] == 1:
                work.pop(0)
                computed.append(g)
            g_left[g] -= 1

    g_left = [4] * len(groups)
    pass_on(0)
    rows[0, t] = fb[me]
    row_scales()
    for i in range(soon, n):
        dispatch(i)
    lag = 3
    for i in range(1, n + lag):
        if i < n:
            pass_on(i)
        if i == min(3, n - 1):
            pltpu.make_async_copy(wgud, wgud, wsem.at[1]).wait()
            arrived(scb.at[0 : n - 1], rsc.at[0])
        one_stage()
        if i >= lag:
            pass_over(i - lag)
            for g, group in enumerate(groups):
                if group[-1] == i - lag:
                    work.append((g, experts(g)))
        one_stage()
    while work:
        one_stage()
        if returned:
            over_y(returned.pop(0))
    for g in computed:
        back(g)
    for i in returned:
        over_y(i)
    arrived(r5.at[0 : n - 1], q5.at[0])

    finished = mid[...] + mm(wcomb[...], r5[...].reshape(n * cap, cw), 1, 0)
    outc[...] = finished.astype(BF16).reshape(nt, rows_here, cw)
    for i in range(1, nt):
        p = lax.rem(t + i, nt)
        send(outc.at[p], fin.at[t], sf.at[0], rf.at[0], {"tp": p})
    fin[t] = outc[t]
    arrived(fin.at[0 : nt - 1], rf.at[0])
    for p in range(nt):
        out[:, p * cw : (p + 1) * cw] = fin[p]
    departed(decall.at[:, 0 : size - 1], sd.at[0])
    departed(sbuf.at[:, 0 : size - 1], sa.at[0])
    departed(cbuf.at[:, 0 : size - 1], sb.at[0])
    departed(scols.at[0 : nt - 1], sst.at[0])
    departed(p1, sp1.at[0])
    departed(ph.at[0 : ny - 1], sp2.at[0])
    departed(squares.at[0 : nt - 1], su.at[0])
    departed(sca.at[0 : n - 1], ssc.at[0])
    departed(fb.at[0 : n - 1], sx.at[0])
    departed(hy.at[:, 0 : ny - 1], sy.at[0])
    departed(r4, sxc.at[0])
    departed(r4, s4.at[0])
    departed(hy.at[:, 0 : ny - 1], s6.at[0])
    departed(hb.at[0 : n - 1], s5.at[0])
    departed(outc.at[0 : nt - 1], sf.at[0])

    @pl.when(team < teams - 1)
    def _():
        departed(tsend, stt.at[0])


def solution(mesh):
    n, nt = mesh.shape["sp"], mesh.shape["tp"]
    ny = nt // 2

    def body(
        stream_in, queries, key_rows, values, decay_low, decay_matrix, decay_bias, decay_shift,
        head_gain, output_matrix, feed_gain, routes, route_weights, expert_gate, specialist_widen,
        expert_down,
    ):
        length, keys = queries.shape
        vals = values.shape[1]
        rows_here, width = stream_in.shape
        hidden = expert_gate.shape[2]
        cap = nt * max(1, TOP * length // (n * nt))
        cw = width // nt
        sides = cw // min(256, cw)
        step = max(1, min(n, 256 // cap))
        groups = n // step + 1
        size = next(x for x in ((4, 2, 1) if n > 8 else (2, 1)) if n % x == 0)
        pieces = (HV // size) // max(16, HV // size // PIECES)
        heads = keys // HK
        blocks = length // BLK
        vm = pltpu.VMEM
        dma = pltpu.SemaphoreType.DMA
        scratch = [
            vm((length, keys), F32), vm((max(1, blocks - 1), HV, keys), BF16),
            *[vm((heads, size, HV // size, HK), BF16)] * 4,
            *[vm((heads, HV // size, HK), BF16)] * 2,
            vm((heads, 1, HK), F32), vm((heads, size, 1, HK), F32),
            vm((length, vals), F32), vm((length, keys), BF16),
            vm(output_matrix.shape, BF16), vm((3, hidden, width), BF16), vm((length, vals), BF16),
            vm((nt, rows_here, cw), BF16), vm((ny, 2, length, cw), BF16), *[vm((ny, length, cw), BF16)] * 3,
            vm((length, cw), F32), vm((nt, 1, length), F32),
            vm((n * cap, length), BF16), vm((length, n * cap), BF16),
            vm((n, 1, 128), F32), vm((n, 1, 128), F32),
            vm((n, cap, cw), BF16), vm((n, nt, cap, cw), BF16),
            vm((step * cap, hidden), F32), vm((step * cap, hidden), BF16),
            vm((n, ny, 2, cap, cw), BF16), *[vm((n, ny, cap, cw), BF16)] * 3,
            vm((n, cap, cw), BF16), vm((n, cap, cw), BF16),
            vm((nt, rows_here, cw), BF16), vm((nt, rows_here, cw), BF16),
            dma((2,)),
            dma((1,)), dma((heads, pieces)), dma((1,)), dma((heads,)),
            dma((1,)), dma((heads,)), dma((1,)), dma((heads, pieces)),
            dma((1,)), dma((1,)), dma((1,)), dma((sides, ny)), dma((1,)), dma((sides, ny)),
            dma((1,)), dma((1,)), dma((1,)), dma((1,)),
            dma((1,)), dma((n,)), dma((1,)), dma((n, ny - 1)), dma((1,)), dma((groups,)),
            dma((1,)), dma((groups,)), dma((1,)), dma((n, ny - 1)), dma((1,)), dma((1,)),
            dma((1,)), dma((1,)),
        ]
        near = pl.BlockSpec(memory_space=pltpu.VMEM)
        far = pl.BlockSpec(memory_space=pl.ANY)
        return pl.pallas_call(
            functools.partial(layer_kernel, n, nt, cap, size),
            out_shape=jax.ShapeDtypeStruct((rows_here, width), BF16),
            in_specs=[near] * 9 + [far] + [near] * 3 + [far] * 3,
            out_specs=near,
            scratch_shapes=scratch,
            compiler_params=pltpu.CompilerParams(
                collective_id=0, has_side_effects=True, vmem_limit_bytes=64_000_000
            ),
            name="layer",
        )(
            stream_in, queries, key_rows, values, decay_low.T, decay_matrix, decay_bias.reshape(1, -1),
            decay_shift.T, head_gain.reshape(1, -1), output_matrix, feed_gain.reshape(1, -1), routes.T,
            route_weights.T, expert_gate.swapaxes(1, 2), specialist_widen.swapaxes(1, 2), expert_down,
        )

    return jax.shard_map(
        body,
        mesh=mesh,
        in_specs=(
            P(("sp", "tp"), None), P("sp", "tp"), P("sp", "tp"), P("sp", "tp"), P("sp", None),
            P(None, "tp"), P("tp"), P("sp", "tp"), P(), P("tp", None), P(), P("sp", None),
            P("sp", None), P("sp", None, "tp"), P("sp", None, "tp"), P("sp", "tp", None),
        ),
        out_specs=P(("sp", "tp"), None),
        check_vma=False,
    )
```

```python
import functools

import jax
import jax.numpy as jnp
from jax import lax
from jax.experimental import pallas as pl
from jax.experimental.pallas import tpu as pltpu
from jax.sharding import PartitionSpec as P

HK = 256
HV = 512
TOP = 2
PIECES = 4
BLK = 128
TEMPER = 16.0
EPSILON = 1e-06
HIGHEST = lax.Precision.HIGHEST
MESH = pl.DeviceIdType.MESH
F32 = jnp.float32
BF16 = jnp.bfloat16


def mm(a, b, ca, cb, precision=None):
    return lax.dot_general(
        a, b, (((ca,), (cb,)), ((), ())), preferred_element_type=F32, precision=precision
    )


def remote(src, dst, send, recv, target):
    return pltpu.make_async_remote_copy(
        src_ref=src, dst_ref=dst, send_sem=send, recv_sem=recv, device_id=target, device_id_type=MESH
    )


def layer_kernel(
    n, nt, cap, size,
    stream_in, q_in, k_in, v_in, low_in, mat_in, bias_in, shift_in, gain_in, wout, fgain_in, routes_in,
    rweights_in, wgate, wup, wdown,
    out,
    stream, q, k, v, low, mat, bias, shift, gain, fgain, routes, rweights,
    ins, prior, sbuf, rbuf, cbuf, carry, tsend, trecv, dec, decall, acc, qs,
    wo, wgud, wt, mixed,
    scols, prod, p1, ph, p2, mid, selt, wcomb, sca, scb,
    fb, rows, gates, hiddens, pb, r4, hy, r6, hb, r5, outc, fin,
    wsem, lsem, sa, ra, sd, rd, sb, rb, stt, rtt, sst, rst, sp1, rp1, sp2, rp2, ssc, rsc,
    sx, rx, sy, ry, sxc, rxc, s4, q4, s6, q6, s5, q5, sf, rf,
):
    me = lax.axis_index("sp")
    t = lax.axis_index("tp")
    y = t // 2
    c = lax.rem(t, 2)
    ny = nt // 2
    mine, team, teams = lax.rem(me, size), me // size, n // size
    first_one = team * size
    partner = {"tp": 2 * y + 1 - c}
    length = q.shape[0]
    heads = q.shape[1] // HK
    blocks = length // BLK
    width = stream.shape[1]
    rows_here = stream.shape[0]
    cw = width // nt
    tile = min(256, cw)
    sides = [slice(f * tile, (f + 1) * tile) for f in range(cw // tile)]
    high = HV // size
    piece = max(16, high // PIECES)
    pieces = [slice(a, a + piece) for a in range(0, high, piece)]

    def send(*args):
        remote(*args).start()

    def arrived(ref, semaphore):
        remote(ref, ref, semaphore, semaphore, partner).wait_recv()

    def departed(ref, semaphore):
        remote(ref, ref, semaphore, semaphore, partner).wait_send()

    def columns(p, f=0, wide=tile):
        return pl.ds(pl.multiple_of(p * cw + f * tile, tile), wide)

    total_devices = n * nt
    rank = me * nt + t
    barrier = pltpu.get_barrier_semaphore()

    @pl.loop(1, total_devices)
    def _(i):
        other = lax.rem(rank + i, total_devices)
        there = {"sp": other // nt, "tp": lax.rem(other, nt)}
        pl.semaphore_signal(barrier, inc=1, device_id=there, device_id_type=MESH)

    loads = [
        pltpu.make_async_copy(source, target, lsem.at[i])
        for i, (source, target) in enumerate((
            (low_in, low), (mat_in, mat), (bias_in, bias), (shift_in, shift), (k_in, k), (v_in, v),
            (stream_in, stream), (q_in, q), (routes_in, routes), (rweights_in, rweights), (gain_in, gain),
            (fgain_in, fgain),
        ))
    ]
    for load in loads:
        load.start()
    load_out = pltpu.make_async_copy(wout, wo, wsem.at[0])
    load_out.start()
    for i, weight in enumerate((wgate, wup, wdown)):
        pltpu.make_async_copy(weight.at[0], wgud.at[i], wsem.at[1]).start()

    row_id = lax.broadcasted_iota(jnp.int32, (BLK, BLK), 0)
    col_id = lax.broadcasted_iota(jnp.int32, (BLK, BLK), 1)
    causal = row_id >= col_id
    tril = causal.astype(F32)

    for load in loads[:4]:
        load.wait()
    shifts = shift[...].T

    for h in range(heads):
        ks, vs = slice(h * HK, (h + 1) * HK), slice(h * HV, (h + 1) * HV)
        pre = mm(low[...], mat[:, ks], 0, 0) + bias[:, ks]
        logged = (jnp.minimum(pre, 0.0) - jnp.log1p(jnp.exp(-jnp.abs(pre)))) / TEMPER + shifts[:, h : h + 1]
        if h == 0:
            for load in loads[4:6]:
                load.wait()
        whole = None
        state = None
        for b in range(blocks):
            at = slice(b * BLK, (b + 1) * BLK)
            inside = mm(tril, logged[at], 1, 0, HIGHEST)
            ins[at, ks] = inside
            last = inside[BLK - 1 : BLK, :]
            whole = last if whole is None else whole + last
            end = (k[at, ks].astype(F32) * jnp.exp(last - inside)).astype(BF16)
            added = mm(v[at, vs], end, 0, 0)
            state = added if state is None else state * jnp.exp(last) + added
            if b < blocks - 1:
                prior[b, :, ks] = state.astype(BF16)
        sbuf[h] = state.astype(BF16).reshape(size, HV // size, HK)
        dec[h] = jnp.exp(whole)
        if h == 0:
            pl.semaphore_wait(barrier, total_devices - 1)
        for i in range(1, size):
            to = lax.rem(mine + i, size)
            send(dec.at[h], decall.at[h, mine], sd.at[0], rd.at[h], {"sp": first_one + to})
        for p, part in enumerate(pieces):
            for i in range(1, size):
                to = lax.rem(mine + i, size)
                send(
                    sbuf.at[h, to, part], rbuf.at[h, mine, part], sa.at[0], ra.at[h, p], {"sp": first_one + to}
                )
        rbuf[h, mine] = sbuf[h, mine]
        decall[h, mine] = dec[h]

    for load in loads[6:]:
        load.wait()
    for i in range(1, nt):
        to = lax.rem(t + i, nt)
        send(stream.at[:, columns(to, 0, cw)], scols.at[t], sst.at[0], rst.at[0], {"tp": to})
    scols[t] = stream[:, columns(t, 0, cw)]

    turns = [(j, slice(a, a + 256)) for j in range(2) for a in range(0, width, 256)]
    onward = {"sp": lax.rem(me + size, n)}
    for h in range(heads):
        ks, vs = slice(h * HK, (h + 1) * HK), slice(h * HV, (h + 1) * HV)
        arrived(decall.at[h, 0 : size - 1], rd.at[h])
        for p, part in enumerate(pieces):
            arrived(rbuf.at[h, 0 : size - 1, part], ra.at[h, p])
            link = remote(tsend.at[h, part], trecv.at[h, part], stt.at[0], rtt.at[h, p], onward)

            @pl.when(team > 0)
            def _():
                link.wait_recv()

            @pl.when(team == 0)
            def _():
                trecv[h, part] = jnp.zeros_like(trecv[h, part])

            total = trecv[h, part].astype(F32)
            for j in range(size):
                cbuf[h, j, part] = total.astype(BF16)
                total = total * decall[h, j] + rbuf[h, j, part].astype(F32)

            @pl.when(team < teams - 1)
            def _():
                tsend[h, part] = total.astype(BF16)
                link.start()

            for i in range(1, size):
                j = lax.rem(mine + i, size)
                send(cbuf.at[h, j, part], carry.at[h, mine, part], sb.at[0], rb.at[h], {"sp": first_one + j})
        carry[h, mine] = cbuf[h, mine]

        passed = None
        for b in range(blocks):
            at = slice(b * BLK, (b + 1) * BLK)
            inside = ins[at, ks]
            last = inside[BLK - 1 : BLK, :]
            centre = last * 0.5
            qf = q[at, ks].astype(F32) * HK ** (-0.5)
            sq = (qf * jnp.exp(inside - centre)).astype(BF16)
            sk = (k[at, ks].astype(F32) * jnp.exp(centre - inside)).astype(BF16)
            scores = jnp.where(causal, mm(sq, sk, 1, 1), 0.0).astype(BF16)
            local = mm(scores, v[at, vs], 1, 0)
            full = inside if passed is None else inside + passed
            qs[at, ks] = (qf * jnp.exp(full)).astype(BF16)
            if b > 0:
                local = local + mm((qf * jnp.exp(inside)).astype(BF16), prior[b - 1, :, ks], 1, 1)
            passed = last if passed is None else passed + last
            acc[at, vs] = local
        if h == 0:
            pltpu.make_async_copy(wgud, wgud, wsem.at[1]).wait()
        if h < max(1, heads - 1):
            for j, at in turns[h :: max(1, heads - 1)]:
                wt[j, at, :] = wgud[j, :, at].T
        if h == min(1, heads - 1):
            lane = lax.broadcasted_iota(jnp.int32, (length, n), 1).astype(F32)
            named = routes[...].astype(F32).T
            shares = rweights[...].T
            first_named = (named[:, 0:1] == lane).astype(F32)
            second_named = (named[:, 1:2] == lane).astype(F32)
            earlier = (
                lax.broadcasted_iota(jnp.int32, (length, length), 0)
                > lax.broadcasted_iota(jnp.int32, (length, length), 1)
            ).astype(BF16)
            counts = mm(earlier, (first_named + second_named).astype(BF16), 1, 0)
            slot_lane = lax.broadcasted_iota(jnp.int32, (length, n * cap), 1).astype(F32)
            chosen = jnp.zeros((length, n * cap), F32)
            weighted = jnp.zeros((length, n * cap), F32)
            for j, mask in enumerate((first_named, second_named)):
                rank = jnp.sum(counts * mask, axis=1, keepdims=True)
                place = jnp.where(rank < cap, named[:, j : j + 1] * cap + rank, -1.0)
                hit = place == slot_lane
                chosen = chosen + jnp.where(hit, 1.0, 0.0)
                weighted = weighted + jnp.where(hit, shares[:, j : j + 1], 0.0)
            selt[...] = chosen.T.astype(BF16)
            wcomb[...] = weighted.astype(BF16)
            sca[...] = jnp.zeros_like(sca)


    for h in range(heads):
        ks, vs = slice(h * HK, (h + 1) * HK), slice(h * HV, (h + 1) * HV)
        arrived(carry.at[h, 0 : size - 1], rb.at[h])
        x = acc[:, vs] + mm(qs[:, ks], carry[h].reshape(HV, HK), 1, 1)
        scale = lax.rsqrt(jnp.mean(x * x, axis=-1, keepdims=True) + EPSILON)
        mixed[:, vs] = (x * scale * gain[...]).astype(BF16)

    load_out.wait()

    def first(to, f):
        at = sides[f]
        return remote(
            prod.at[to, 1 - c, :, at], p1.at[to, :, at], sp1.at[0], rp1.at[f, to], partner
        )

    def second(to, slot, f):
        at = sides[f]
        return remote(
            ph.at[to, :, at], p2.at[slot, :, at], sp2.at[0], rp2.at[f, slot], {"tp": 2 * to + c}
        )

    def project(to, core, f):
        prod[to, core, :, sides[f]] = mm(mixed[...], wo[:, columns(2 * to + core, f)], 1, 0).astype(BF16)

    for i in range(1, ny + 1):
        to = lax.rem(y + i, ny)
        for f in range(len(sides)):
            project(to, 1 - c, f)
            first(to, f).start()
        for f in range(len(sides)):
            project(to, c, f)
        if i < ny:
            for f, at in enumerate(sides):
                first(to, f).wait_recv()
                ph[to, :, at] = (prod[to, c, :, at].astype(F32) + p1[to, :, at].astype(F32)).astype(BF16)
                second(to, y, f).start()

    arrived(scols.at[0 : nt - 1], rst.at[0])
    square = jnp.zeros((length, 1), F32)
    for f, at in enumerate(sides):
        first(y, f).wait_recv()
        total = prod[y, c, :, at].astype(F32) + p1[y, :, at].astype(F32)
        for i in range(1, ny):
            to = lax.rem(y + i, ny)
            second(to, to, f).wait_recv()
            total = total + p2[to, :, at].astype(F32)
        x = scols[:, :, at].reshape(length, tile).astype(F32) + total
        mid[:, at] = x
        square = square + jnp.sum(x * x, axis=1, keepdims=True)
        if f == len(sides) - 1:
            row = jnp.broadcast_to(square, (length, 128)).T[0:8, :]
            upper = row.astype(BF16).astype(F32)
            middle = (row - upper).astype(BF16).astype(F32)
            line = lax.broadcasted_iota(jnp.int32, (8, length), 0)
            parts = jnp.where(line == 0, upper, jnp.where(line == 1, middle, jnp.where(line == 2, row - upper - middle, 0.0)))
            slot_squares = jnp.sum(mm(parts.astype(BF16), selt[...], 1, 1), axis=0, keepdims=True)
            for e in range(n):
                sca[e, :, 0:cap] = slot_squares[:, e * cap : (e + 1) * cap]
            for i in range(n):
                to = lax.rem(me + i, n)
                for j in range(0 if i else 1, nt):
                    send(
                        sca.at[to], scb.at[i * nt + t], ssc.at[0], rsc.at[0], {"sp": to, "tp": lax.rem(t + j, nt)}
                    )
            scb[t] = sca[me]
        picked = mm(selt[...], (x * fgain[:, columns(t, f)]).astype(BF16), 1, 0)
        fb[:, :, at] = picked.astype(BF16).reshape(n, cap, tile)
        for i in range(1, n):
            to = lax.rem(me + i, n)
            send(fb.at[to, :, at], rows.at[i, t, :, at], sx.at[0], rx.at[i], {"sp": to})

    step = max(1, min(n, 256 // cap))
    groups = [range(a, a + step) for a in range(0, n, step)]
    if step > 1:
        first_half = groups[-1][: step // 2]
        groups = groups[:-1] + [first_half, groups[-1][step // 2 :]]

    def group_of(i):
        return next(g for g, group in enumerate(groups) if i in group)

    def pass_on(i):
        if i > 0:
            arrived(rows.at[i, t], rx.at[i])
        block = fb.at[me] if i == 0 else rows.at[i, t]
        for d in range(1, ny):
            send(block, rows.at[i, t], sy.at[0], ry.at[i, d - 1], {"tp": 2 * lax.rem(y + d, ny) + c})
        send(block, rows.at[i, t], sxc.at[0], rxc.at[group_of(i)], partner)

    def pass_over(i):
        for d in range(1, ny):
            other = lax.rem(y + ny - d, ny)
            block = rows.at[i, 2 * other + c]
            arrived(block, ry.at[i, d - 1])
            send(block, block, sxc.at[0], rxc.at[group_of(i)], partner)

    def experts(g):
        group = groups[g]
        span = slice(group[0], group[-1] + 1)
        size_here = len(group) * cap
        arrived(rows.at[span, 0:ny], rxc.at[g])
        parts = [rows[span, p].reshape(size_here, cw) for p in range(nt)]
        gates[0:size_here] = mm(jnp.concatenate(parts, axis=1), wt[0], 1, 0)
        yield
        parts = [rows[span, p].reshape(size_here, cw) for p in range(nt)]
        lifted = mm(jnp.concatenate(parts, axis=1), wt[1], 1, 0)
        if g == 0:
            arrived(scb.at[0 : n * nt - 1], rsc.at[0])
        scales = []
        for i in group:
            total = jnp.sum(scb[i * nt : (i + 1) * nt], axis=0)
            line = lax.rsqrt(total / width + EPSILON)
            scales.append(jnp.broadcast_to(line, (8, 128)).T[0:cap, 0:1])
        scale = jnp.concatenate(scales, axis=0)
        lifted = lifted * scale
        gated = gates[0:size_here] * scale
        hiddens[0:size_here] = (gated * jax.nn.sigmoid(gated) * lifted).astype(BF16)
        yield
        for core in (1 - c, c):
            for d in range(ny):
                piece = mm(hiddens[0:size_here], wgud[2, :, columns(2 * d + core, 0, cw)], 1, 0).astype(BF16)
                pb[span, d, core] = piece.reshape(len(group), cap, cw)
            if core is not c:
                for i in group:
                    for d in range(ny):
                        send(pb.at[i, d, core], r4.at[i, d], s4.at[0], q4.at[g], partner)
            yield

    def over_core(i):
        for d in range(1, ny):
            other = lax.rem(y + d, ny)
            hy[i, other] = (pb[i, other, c].astype(F32) + r4[i, other].astype(F32)).astype(BF16)
            send(hy.at[i, other], r6.at[i, d], s6.at[0], q6.at[i, d - 1], {"tp": 2 * other + c})

    def over_y(i):
        both = pb[i, y, c].astype(F32) + r4[i, y].astype(F32)
        for d in range(1, ny):
            arrived(r6.at[i, d], q6.at[i, d - 1])
            both = both + r6[i, d].astype(F32)
        if i == 0:
            r5[me] = both.astype(BF16)
        else:
            j = lax.rem(me + n - i, n)
            hb[i] = both.astype(BF16)
            send(hb.at[i], r5.at[me], s5.at[0], q5.at[0], {"sp": j})

    work, computed, returned = [], [], []

    def back(g):
        arrived(r4.at[groups[g][0] : groups[g][-1] + 1], q4.at[g])
        for i in groups[g]:
            over_core(i)
            returned.append(i)

    def one_stage():
        if work:
            if computed:
                back(computed.pop(0))
            g, stages = work[0]
            next(stages)
            if g_left[g] == 1:
                work.pop(0)
                computed.append(g)
            g_left[g] -= 1

    g_left = [4] * len(groups)
    pass_on(0)
    rows[0, t] = fb[me]
    lag = 3
    for i in range(1, n + lag):
        if i < n:
            pass_on(i)
        one_stage()
        if i >= lag:
            pass_over(i - lag)
            for g, group in enumerate(groups):
                if group[-1] == i - lag:
                    work.append((g, experts(g)))
        one_stage()
    while work:
        one_stage()
        if returned:
            over_y(returned.pop(0))
    for g in computed:
        back(g)
    for i in returned:
        over_y(i)
    arrived(r5.at[0 : n - 1], q5.at[0])

    finished = mid[...] + mm(wcomb[...], r5[...].reshape(n * cap, cw), 1, 0)
    outc[...] = finished.astype(BF16).reshape(nt, rows_here, cw)
    for i in range(1, nt):
        p = lax.rem(t + i, nt)
        send(outc.at[p], fin.at[t], sf.at[0], rf.at[0], {"tp": p})
    fin[t] = outc[t]
    arrived(fin.at[0 : nt - 1], rf.at[0])
    for p in range(nt):
        out[:, p * cw : (p + 1) * cw] = fin[p]
    departed(decall.at[:, 0 : size - 1], sd.at[0])
    departed(sbuf.at[:, 0 : size - 1], sa.at[0])
    departed(cbuf.at[:, 0 : size - 1], sb.at[0])
    departed(scols.at[0 : nt - 1], sst.at[0])
    departed(p1, sp1.at[0])
    departed(ph.at[0 : ny - 1], sp2.at[0])
    departed(scb.at[0 : n * nt - 1], ssc.at[0])
    departed(fb.at[0 : n - 1], sx.at[0])
    departed(hy.at[:, 0 : ny - 1], sy.at[0])
    departed(r4, sxc.at[0])
    departed(r4, s4.at[0])
    departed(hy.at[:, 0 : ny - 1], s6.at[0])
    departed(hb.at[0 : n - 1], s5.at[0])
    departed(outc.at[0 : nt - 1], sf.at[0])

    @pl.when(team < teams - 1)
    def _():
        departed(tsend, stt.at[0])


def solution(mesh):
    n, nt = mesh.shape["sp"], mesh.shape["tp"]
    ny = nt // 2

    def body(
        stream_in, queries, key_rows, values, decay_low, decay_matrix, decay_bias, decay_shift,
        head_gain, output_matrix, feed_gain, routes, route_weights, expert_gate, specialist_widen,
        expert_down,
    ):
        length, keys = queries.shape
        vals = values.shape[1]
        rows_here, width = stream_in.shape
        hidden = expert_gate.shape[2]
        cap = nt * max(1, TOP * length // (n * nt))
        cw = width // nt
        sides = cw // min(256, cw)
        step = max(1, min(n, 256 // cap))
        groups = n // step + 1
        size = next(x for x in ((4, 2, 1) if n > 8 else (2, 1)) if n % x == 0)
        pieces = (HV // size) // max(16, HV // size // PIECES)
        heads = keys // HK
        blocks = length // BLK
        vm = pltpu.VMEM
        dma = pltpu.SemaphoreType.DMA
        given = [
            stream_in, queries, key_rows, values, decay_low.T, decay_matrix, decay_bias.reshape(1, -1),
            decay_shift.T, head_gain.reshape(1, -1), output_matrix, feed_gain.reshape(1, -1), routes.T,
            route_weights.T, expert_gate.swapaxes(1, 2), specialist_widen.swapaxes(1, 2), expert_down,
        ]
        scratch = [
            *[vm(given[i].shape, given[i].dtype) for i in (0, 1, 2, 3, 4, 5, 6, 7, 8, 10, 11, 12)],
            vm((length, keys), F32), vm((max(1, blocks - 1), HV, keys), BF16),
            *[vm((heads, size, HV // size, HK), BF16)] * 4,
            *[vm((heads, HV // size, HK), BF16)] * 2,
            vm((heads, 1, HK), F32), vm((heads, size, 1, HK), F32),
            vm((length, vals), F32), vm((length, keys), BF16),
            vm(output_matrix.shape, BF16), vm((3, hidden, width), BF16), vm((2, width, hidden), BF16), vm((length, vals), BF16),
            vm((nt, rows_here, cw), BF16), vm((ny, 2, length, cw), BF16), *[vm((ny, length, cw), BF16)] * 3,
            vm((length, cw), F32),
            vm((n * cap, length), BF16), vm((length, n * cap), BF16),
            vm((n, 1, 128), F32), vm((n * nt, 1, 128), F32),
            vm((n, cap, cw), BF16), vm((n, nt, cap, cw), BF16),
            vm((step * cap, hidden), F32), vm((step * cap, hidden), BF16),
            vm((n, ny, 2, cap, cw), BF16), *[vm((n, ny, cap, cw), BF16)] * 3,
            vm((n, cap, cw), BF16), vm((n, cap, cw), BF16),
            vm((nt, rows_here, cw), BF16), vm((nt, rows_here, cw), BF16),
            dma((2,)), dma((12,)),
            dma((1,)), dma((heads, pieces)), dma((1,)), dma((heads,)),
            dma((1,)), dma((heads,)), dma((1,)), dma((heads, pieces)),
            dma((1,)), dma((1,)), dma((1,)), dma((sides, ny)), dma((1,)), dma((sides, ny)),
            dma((1,)), dma((1,)),
            dma((1,)), dma((n,)), dma((1,)), dma((n, ny - 1)), dma((1,)), dma((groups,)),
            dma((1,)), dma((groups,)), dma((1,)), dma((n, ny - 1)), dma((1,)), dma((1,)),
            dma((1,)), dma((1,)),
        ]
        near = pl.BlockSpec(memory_space=pltpu.VMEM)
        far = pl.BlockSpec(memory_space=pl.ANY)
        return pl.pallas_call(
            functools.partial(layer_kernel, n, nt, cap, size),
            out_shape=jax.ShapeDtypeStruct((rows_here, width), BF16),
            in_specs=[far] * 16,
            out_specs=near,
            scratch_shapes=scratch,
            compiler_params=pltpu.CompilerParams(
                collective_id=0, has_side_effects=True, vmem_limit_bytes=64_000_000
            ),
            name="layer",
        )(*given)

    return jax.shard_map(
        body,
        mesh=mesh,
        in_specs=(
            P(("sp", "tp"), None), P("sp", "tp"), P("sp", "tp"), P("sp", "tp"), P("sp", None),
            P(None, "tp"), P("tp"), P("sp", "tp"), P(), P("tp", None), P(), P("sp", None),
            P("sp", None), P("sp", None, "tp"), P("sp", None, "tp"), P("sp", "tp", None),
        ),
        out_specs=P(("sp", "tp"), None),
        check_vma=False,
    )
```

```python
import functools

import jax
import jax.numpy as jnp
from jax import lax
from jax.experimental import pallas as pl
from jax.experimental.pallas import tpu as pltpu
from jax.sharding import PartitionSpec as P

HK = 256
HV = 512
TOP = 2
PIECES = 4
BLK = 128
TEMPER = 16.0
EPSILON = 1e-06
HIGHEST = lax.Precision.HIGHEST
MESH = pl.DeviceIdType.MESH
F32 = jnp.float32
BF16 = jnp.bfloat16


def mm(a, b, ca, cb, precision=None):
    return lax.dot_general(
        a, b, (((ca,), (cb,)), ((), ())), preferred_element_type=F32, precision=precision
    )


def remote(src, dst, send, recv, target):
    return pltpu.make_async_remote_copy(
        src_ref=src, dst_ref=dst, send_sem=send, recv_sem=recv, device_id=target, device_id_type=MESH
    )


def layer_kernel(
    n, nt, cap, size,
    stream_in, q_in, k_in, v_in, low_in, mat_in, bias_in, shift_in, gain_in, wout, fgain_in, routes_in,
    rweights_in, wgate, wup, wdown,
    out,
    stream, q, k, v, low, mat, bias, shift, gain, fgain, routes, rweights,
    ins, prior, sbuf, rbuf, cbuf, carry, tsend, trecv, dec, decall, acc, qs,
    wo, wgud, wt, mixed,
    scols, prod, p1, ph, p2, mid, selt, wcomb, sca, scb,
    fb, rows, gates, hiddens, pb, r4, hy, r6, hb, r5, outc, fin,
    wsem, lsem, sa, ra, sd, rd, sb, rb, stt, rtt, sst, rst, sp1, rp1, sp2, rp2, ssc, rsc,
    sx, rx, sy, ry, sxc, rxc, s4, q4, s6, q6, s5, q5, sf, rf,
):
    me = lax.axis_index("sp")
    t = lax.axis_index("tp")
    y = t // 2
    c = lax.rem(t, 2)
    ny = nt // 2
    mine, team, teams = lax.rem(me, size), me // size, n // size
    first_one = team * size
    partner = {"tp": 2 * y + 1 - c}
    length = q.shape[0]
    heads = q.shape[1] // HK
    blocks = length // BLK
    width = stream.shape[1]
    rows_here = stream.shape[0]
    cw = width // nt
    tile = min(256, cw)
    sides = [slice(f * tile, (f + 1) * tile) for f in range(cw // tile)]
    high = HV // size
    piece = max(16, high // PIECES)
    pieces = [slice(a, a + piece) for a in range(0, high, piece)]

    def send(*args):
        remote(*args).start()

    def arrived(ref, semaphore):
        remote(ref, ref, semaphore, semaphore, partner).wait_recv()

    def departed(ref, semaphore):
        remote(ref, ref, semaphore, semaphore, partner).wait_send()

    def columns(p, f=0, wide=tile):
        return pl.ds(pl.multiple_of(p * cw + f * tile, tile), wide)

    total_devices = n * nt
    rank = me * nt + t
    barrier = pltpu.get_barrier_semaphore()

    @pl.loop(1, total_devices)
    def _(i):
        other = lax.rem(rank + i, total_devices)
        there = {"sp": other // nt, "tp": lax.rem(other, nt)}
        pl.semaphore_signal(barrier, inc=1, device_id=there, device_id_type=MESH)

    loads = [
        pltpu.make_async_copy(source, target, lsem.at[i])
        for i, (source, target) in enumerate((
            (low_in, low), (mat_in, mat), (bias_in, bias), (shift_in, shift), (k_in, k), (v_in, v),
            (stream_in, stream), (q_in, q), (routes_in, routes), (rweights_in, rweights), (gain_in, gain),
            (fgain_in, fgain),
        ))
    ]
    for load in loads:
        load.start()
    load_out = pltpu.make_async_copy(wout, wo, wsem.at[0])
    load_out.start()
    for i, weight in enumerate((wgate, wup, wdown)):
        pltpu.make_async_copy(weight.at[0], wgud.at[i], wsem.at[1]).start()

    row_id = lax.broadcasted_iota(jnp.int32, (BLK, BLK), 0)
    col_id = lax.broadcasted_iota(jnp.int32, (BLK, BLK), 1)
    causal = row_id >= col_id
    tril = causal.astype(F32)

    for load in loads[:4]:
        load.wait()
    shifts = shift[...].T

    for h in range(heads):
        ks, vs = slice(h * HK, (h + 1) * HK), slice(h * HV, (h + 1) * HV)
        pre = mm(low[...], mat[:, ks], 0, 0) + bias[:, ks]
        logged = (jnp.minimum(pre, 0.0) - jnp.log1p(jnp.exp(-jnp.abs(pre)))) / TEMPER + shifts[:, h : h + 1]
        if h == 0:
            for load in loads[4:6]:
                load.wait()
        whole = None
        state = None
        for b in range(blocks):
            at = slice(b * BLK, (b + 1) * BLK)
            inside = mm(tril, logged[at], 1, 0, HIGHEST)
            ins[at, ks] = inside
            last = inside[BLK - 1 : BLK, :]
            whole = last if whole is None else whole + last
            end = (k[at, ks].astype(F32) * jnp.exp(last - inside)).astype(BF16)
            added = mm(v[at, vs], end, 0, 0)
            state = added if state is None else state * jnp.exp(last) + added
            if b < blocks - 1:
                prior[b, :, ks] = state.astype(BF16)
        sbuf[h] = state.astype(BF16).reshape(size, HV // size, HK)
        dec[h] = jnp.exp(whole)
        if h == 0:
            pl.semaphore_wait(barrier, total_devices - 1)
        for i in range(1, size):
            to = lax.rem(mine + i, size)
            send(dec.at[h], decall.at[h, mine], sd.at[0], rd.at[h], {"sp": first_one + to})
        for p, part in enumerate(pieces):
            for i in range(1, size):
                to = lax.rem(mine + i, size)
                send(
                    sbuf.at[h, to, part], rbuf.at[h, mine, part], sa.at[0], ra.at[h, p], {"sp": first_one + to}
                )
        rbuf[h, mine] = sbuf[h, mine]
        decall[h, mine] = dec[h]

    for load in loads[6:]:
        load.wait()
    for i in range(1, nt):
        to = lax.rem(t + i, nt)
        send(stream.at[:, columns(to, 0, cw)], scols.at[t], sst.at[0], rst.at[0], {"tp": to})
    scols[t] = stream[:, columns(t, 0, cw)]

    turns = [(j, slice(a, a + 256)) for j in range(2) for a in range(0, width, 256)]
    onward = {"sp": lax.rem(me + size, n)}
    for h in range(heads):
        ks, vs = slice(h * HK, (h + 1) * HK), slice(h * HV, (h + 1) * HV)
        arrived(decall.at[h, 0 : size - 1], rd.at[h])
        for p, part in enumerate(pieces):
            arrived(rbuf.at[h, 0 : size - 1, part], ra.at[h, p])
            link = remote(tsend.at[h, part], trecv.at[h, part], stt.at[0], rtt.at[h, p], onward)

            @pl.when(team > 0)
            def _():
                link.wait_recv()

            @pl.when(team == 0)
            def _():
                trecv[h, part] = jnp.zeros_like(trecv[h, part])

            total = trecv[h, part].astype(F32)
            for j in range(size):
                cbuf[h, j, part] = total.astype(BF16)
                total = total * decall[h, j] + rbuf[h, j, part].astype(F32)

            @pl.when(team < teams - 1)
            def _():
                tsend[h, part] = total.astype(BF16)
                link.start()

            for i in range(1, size):
                j = lax.rem(mine + i, size)
                send(cbuf.at[h, j, part], carry.at[h, mine, part], sb.at[0], rb.at[h], {"sp": first_one + j})
        carry[h, mine] = cbuf[h, mine]

        passed = None
        for b in range(blocks):
            at = slice(b * BLK, (b + 1) * BLK)
            inside = ins[at, ks]
            last = inside[BLK - 1 : BLK, :]
            centre = last * 0.5
            qf = q[at, ks].astype(F32) * HK ** (-0.5)
            sq = (qf * jnp.exp(inside - centre)).astype(BF16)
            sk = (k[at, ks].astype(F32) * jnp.exp(centre - inside)).astype(BF16)
            scores = jnp.where(causal, mm(sq, sk, 1, 1), 0.0).astype(BF16)
            local = mm(scores, v[at, vs], 1, 0)
            full = inside if passed is None else inside + passed
            qs[at, ks] = (qf * jnp.exp(full)).astype(BF16)
            if b > 0:
                local = local + mm((qf * jnp.exp(inside)).astype(BF16), prior[b - 1, :, ks], 1, 1)
            passed = last if passed is None else passed + last
            acc[at, vs] = local
        if h == 0:
            pltpu.make_async_copy(wgud, wgud, wsem.at[1]).wait()
        if h < max(1, heads - 1):
            for j, at in turns[h :: max(1, heads - 1)]:
                wt[j, at, :] = wgud[j, :, at].T
        if h == min(1, heads - 1):
            lane = lax.broadcasted_iota(jnp.int32, (length, n), 1).astype(F32)
            named = routes[...].astype(F32).T
            shares = rweights[...].T
            first_named = (named[:, 0:1] == lane).astype(F32)
            second_named = (named[:, 1:2] == lane).astype(F32)
            earlier = (
                lax.broadcasted_iota(jnp.int32, (length, length), 0)
                > lax.broadcasted_iota(jnp.int32, (length, length), 1)
            ).astype(BF16)
            counts = mm(earlier, (first_named + second_named).astype(BF16), 1, 0)
            slot_lane = lax.broadcasted_iota(jnp.int32, (length, n * cap), 1).astype(F32)
            chosen = jnp.zeros((length, n * cap), F32)
            weighted = jnp.zeros((length, n * cap), F32)
            for j, mask in enumerate((first_named, second_named)):
                rank = jnp.sum(counts * mask, axis=1, keepdims=True)
                place = jnp.where(rank < cap, named[:, j : j + 1] * cap + rank, -1.0)
                hit = place == slot_lane
                chosen = chosen + jnp.where(hit, 1.0, 0.0)
                weighted = weighted + jnp.where(hit, shares[:, j : j + 1], 0.0)
            selt[...] = chosen.T.astype(BF16)
            wcomb[...] = weighted.astype(BF16)
            sca[...] = jnp.zeros_like(sca)


    for h in range(heads):
        ks, vs = slice(h * HK, (h + 1) * HK), slice(h * HV, (h + 1) * HV)
        arrived(carry.at[h, 0 : size - 1], rb.at[h])
        x = acc[:, vs] + mm(qs[:, ks], carry[h].reshape(HV, HK), 1, 1)
        scale = lax.rsqrt(jnp.mean(x * x, axis=-1, keepdims=True) + EPSILON)
        mixed[:, vs] = (x * scale * gain[...]).astype(BF16)

    load_out.wait()

    def first(to, f):
        at = sides[f]
        return remote(
            prod.at[to, 1 - c, :, at], p1.at[to, :, at], sp1.at[0], rp1.at[f, to], partner
        )

    def second(to, slot, f):
        at = sides[f]
        return remote(
            ph.at[to, :, at], p2.at[slot, :, at], sp2.at[0], rp2.at[f, slot], {"tp": 2 * to + c}
        )

    def project(to, core, f):
        prod[to, core, :, sides[f]] = mm(mixed[...], wo[:, columns(2 * to + core, f)], 1, 0).astype(BF16)

    for i in range(1, ny + 1):
        to = lax.rem(y + i, ny)
        for f in range(len(sides)):
            project(to, 1 - c, f)
            first(to, f).start()
        for f in range(len(sides)):
            project(to, c, f)
        if i < ny:
            for f, at in enumerate(sides):
                first(to, f).wait_recv()
                ph[to, :, at] = (prod[to, c, :, at].astype(F32) + p1[to, :, at].astype(F32)).astype(BF16)
                second(to, y, f).start()

    arrived(scols.at[0 : nt - 1], rst.at[0])
    square = jnp.zeros((length, 1), F32)
    for f, at in enumerate(sides):
        first(y, f).wait_recv()
        total = prod[y, c, :, at].astype(F32) + p1[y, :, at].astype(F32)
        for i in range(1, ny):
            to = lax.rem(y + i, ny)
            second(to, to, f).wait_recv()
            total = total + p2[to, :, at].astype(F32)
        x = scols[:, :, at].reshape(length, tile).astype(F32) + total
        mid[:, at] = x
        square = square + jnp.sum(x * x, axis=1, keepdims=True)
        if f == len(sides) - 1:
            row = jnp.broadcast_to(square, (length, 128)).T[0:8, :]
            upper = row.astype(BF16).astype(F32)
            middle = (row - upper).astype(BF16).astype(F32)
            line = lax.broadcasted_iota(jnp.int32, (8, length), 0)
            parts = jnp.where(line == 0, upper, jnp.where(line == 1, middle, jnp.where(line == 2, row - upper - middle, 0.0)))
            slot_squares = jnp.sum(mm(parts.astype(BF16), selt[...], 1, 1), axis=0, keepdims=True)
            for e in range(n):
                sca[e, :, 0:cap] = slot_squares[:, e * cap : (e + 1) * cap]
            for i in range(n):
                to = lax.rem(me + i, n)
                for j in range(0 if i else 1, nt):
                    send(
                        sca.at[to], scb.at[me * nt + t], ssc.at[0], rsc.at[0], {"sp": to, "tp": lax.rem(t + j, nt)}
                    )
            scb[me * nt + t] = sca[me]
        picked = mm(selt[...], (x * fgain[:, columns(t, f)]).astype(BF16), 1, 0)
        fb[:, :, at] = picked.astype(BF16).reshape(n, cap, tile)
        for i in range(1, n):
            to = lax.rem(me + i, n)
            send(fb.at[to, :, at], rows.at[me, t, :, at], sx.at[0], rx.at[me], {"sp": to})

    step = max(1, min(n, 256 // cap))
    groups = [range(a, a + step) for a in range(0, n, step)]
    if step > 1:
        first_half = groups[-1][: step // 2]
        groups = groups[:-1] + [first_half, groups[-1][step // 2 :]]

    def group_of(i):
        return next(g for g, group in enumerate(groups) if i in group)

    def group_at(i):
        g = 0
        for group in groups[1:]:
            g = g + (i >= group[0]).astype(jnp.int32)
        return g

    def forward(i, g):
        block = rows.at[i, t]
        for d in range(1, ny):
            send(block, rows.at[i, t], sy.at[0], ry.at[i, d - 1], {"tp": 2 * lax.rem(y + d, ny) + c})
        send(block, rows.at[i, t], sxc.at[0], rxc.at[g], partner)

    def pass_on(i):
        @pl.when(i // size != team)
        def _():
            arrived(rows.at[i, t], rx.at[i])
            forward(i, group_of(i))

    def pass_over(i):
        for d in range(1, ny):
            other = lax.rem(y + ny - d, ny)
            block = rows.at[i, 2 * other + c]
            arrived(block, ry.at[i, d - 1])
            send(block, block, sxc.at[0], rxc.at[group_of(i)], partner)

    def experts(g):
        group = groups[g]
        span = slice(group[0], group[-1] + 1)
        size_here = len(group) * cap
        arrived(rows.at[span, 0:ny], rxc.at[g])
        parts = [rows[span, p].reshape(size_here, cw) for p in range(nt)]
        gates[0:size_here] = mm(jnp.concatenate(parts, axis=1), wt[0], 1, 0)
        yield
        parts = [rows[span, p].reshape(size_here, cw) for p in range(nt)]
        lifted = mm(jnp.concatenate(parts, axis=1), wt[1], 1, 0)
        if g == 0:
            arrived(scb.at[0 : n * nt - 1], rsc.at[0])
        scales = []
        for i in group:
            total = jnp.sum(scb[i * nt : (i + 1) * nt], axis=0)
            line = lax.rsqrt(total / width + EPSILON)
            scales.append(jnp.broadcast_to(line, (8, 128)).T[0:cap, 0:1])
        scale = jnp.concatenate(scales, axis=0)
        lifted = lifted * scale
        gated = gates[0:size_here] * scale
        hiddens[0:size_here] = (gated * jax.nn.sigmoid(gated) * lifted).astype(BF16)
        yield
        for core in (1 - c, c):
            for d in range(ny):
                piece = mm(hiddens[0:size_here], wgud[2, :, columns(2 * d + core, 0, cw)], 1, 0).astype(BF16)
                pb[span, d, core] = piece.reshape(len(group), cap, cw)
            if core is not c:
                for i in group:
                    for d in range(ny):
                        send(pb.at[i, d, core], r4.at[i, d], s4.at[0], q4.at[g], partner)
            yield

    def over_core(i):
        for d in range(1, ny):
            other = lax.rem(y + d, ny)
            hy[i, other] = (pb[i, other, c].astype(F32) + r4[i, other].astype(F32)).astype(BF16)
            send(hy.at[i, other], r6.at[i, d], s6.at[0], q6.at[i, d - 1], {"tp": 2 * other + c})

    def over_y(i):
        both = pb[i, y, c].astype(F32) + r4[i, y].astype(F32)
        for d in range(1, ny):
            arrived(r6.at[i, d], q6.at[i, d - 1])
            both = both + r6[i, d].astype(F32)
        hb[i] = both.astype(BF16)

        @pl.when(i == me)
        def _():
            r5[me] = hb[i]

        @pl.when(i != me)
        def _():
            send(hb.at[i], r5.at[me], s5.at[0], q5.at[0], {"sp": i})


    work, computed, returned = [], [], []

    def back(g):
        arrived(r4.at[groups[g][0] : groups[g][-1] + 1], q4.at[g])
        for i in groups[g]:
            over_core(i)
            returned.append(i)

    def one_stage():
        if work:
            if computed:
                back(computed.pop(0))
            g, stages = work[0]
            next(stages)
            if g_left[g] == 1:
                work.pop(0)
                computed.append(g)
            g_left[g] -= 1

    g_left = [4] * len(groups)
    rows[me, t] = fb[me]
    forward(me, group_at(me))
    for i in range(1, size):
        mate = first_one + lax.rem(mine + i, size)
        arrived(rows.at[mate, t], rx.at[mate])
        forward(mate, group_at(mate))
    lag = 3
    for i in range(n + lag):
        if i < n:
            pass_on(i)
        one_stage()
        if i >= lag:
            pass_over(i - lag)
            for g, group in enumerate(groups):
                if group[-1] == i - lag:
                    work.append((g, experts(g)))
        one_stage()
    while work:
        one_stage()
        if returned:
            over_y(returned.pop(0))
    for g in computed:
        back(g)
    for i in returned:
        over_y(i)
    arrived(r5.at[0 : n - 1], q5.at[0])

    finished = mid[...] + mm(wcomb[...], r5[...].reshape(n * cap, cw), 1, 0)
    outc[...] = finished.astype(BF16).reshape(nt, rows_here, cw)
    for i in range(1, nt):
        p = lax.rem(t + i, nt)
        send(outc.at[p], fin.at[t], sf.at[0], rf.at[0], {"tp": p})
    fin[t] = outc[t]
    arrived(fin.at[0 : nt - 1], rf.at[0])
    for p in range(nt):
        out[:, p * cw : (p + 1) * cw] = fin[p]
    departed(decall.at[:, 0 : size - 1], sd.at[0])
    departed(sbuf.at[:, 0 : size - 1], sa.at[0])
    departed(cbuf.at[:, 0 : size - 1], sb.at[0])
    departed(scols.at[0 : nt - 1], sst.at[0])
    departed(p1, sp1.at[0])
    departed(ph.at[0 : ny - 1], sp2.at[0])
    departed(scb.at[0 : n * nt - 1], ssc.at[0])
    departed(fb.at[0 : n - 1], sx.at[0])
    departed(hy.at[:, 0 : ny - 1], sy.at[0])
    departed(r4, sxc.at[0])
    departed(r4, s4.at[0])
    departed(hy.at[:, 0 : ny - 1], s6.at[0])
    departed(hb.at[0 : n - 1], s5.at[0])
    departed(outc.at[0 : nt - 1], sf.at[0])

    @pl.when(team < teams - 1)
    def _():
        departed(tsend, stt.at[0])


def solution(mesh):
    n, nt = mesh.shape["sp"], mesh.shape["tp"]
    ny = nt // 2

    def body(
        stream_in, queries, key_rows, values, decay_low, decay_matrix, decay_bias, decay_shift,
        head_gain, output_matrix, feed_gain, routes, route_weights, expert_gate, specialist_widen,
        expert_down,
    ):
        length, keys = queries.shape
        vals = values.shape[1]
        rows_here, width = stream_in.shape
        hidden = expert_gate.shape[2]
        cap = nt * max(1, TOP * length // (n * nt))
        cw = width // nt
        sides = cw // min(256, cw)
        step = max(1, min(n, 256 // cap))
        groups = n // step + 1
        size = next(x for x in ((4, 2, 1) if n > 8 else (2, 1)) if n % x == 0)
        pieces = (HV // size) // max(16, HV // size // PIECES)
        heads = keys // HK
        blocks = length // BLK
        vm = pltpu.VMEM
        dma = pltpu.SemaphoreType.DMA
        given = [
            stream_in, queries, key_rows, values, decay_low.T, decay_matrix, decay_bias.reshape(1, -1),
            decay_shift.T, head_gain.reshape(1, -1), output_matrix, feed_gain.reshape(1, -1), routes.T,
            route_weights.T, expert_gate.swapaxes(1, 2), specialist_widen.swapaxes(1, 2), expert_down,
        ]
        scratch = [
            *[vm(given[i].shape, given[i].dtype) for i in (0, 1, 2, 3, 4, 5, 6, 7, 8, 10, 11, 12)],
            vm((length, keys), F32), vm((max(1, blocks - 1), HV, keys), BF16),
            *[vm((heads, size, HV // size, HK), BF16)] * 4,
            *[vm((heads, HV // size, HK), BF16)] * 2,
            vm((heads, 1, HK), F32), vm((heads, size, 1, HK), F32),
            vm((length, vals), F32), vm((length, keys), BF16),
            vm(output_matrix.shape, BF16), vm((3, hidden, width), BF16), vm((2, width, hidden), BF16), vm((length, vals), BF16),
            vm((nt, rows_here, cw), BF16), vm((ny, 2, length, cw), BF16), *[vm((ny, length, cw), BF16)] * 3,
            vm((length, cw), F32),
            vm((n * cap, length), BF16), vm((length, n * cap), BF16),
            vm((n, 1, 128), F32), vm((n * nt, 1, 128), F32),
            vm((n, cap, cw), BF16), vm((n, nt, cap, cw), BF16),
            vm((step * cap, hidden), F32), vm((step * cap, hidden), BF16),
            vm((n, ny, 2, cap, cw), BF16), *[vm((n, ny, cap, cw), BF16)] * 3,
            vm((n, cap, cw), BF16), vm((n, cap, cw), BF16),
            vm((nt, rows_here, cw), BF16), vm((nt, rows_here, cw), BF16),
            dma((2,)), dma((12,)),
            dma((1,)), dma((heads, pieces)), dma((1,)), dma((heads,)),
            dma((1,)), dma((heads,)), dma((1,)), dma((heads, pieces)),
            dma((1,)), dma((1,)), dma((1,)), dma((sides, ny)), dma((1,)), dma((sides, ny)),
            dma((1,)), dma((1,)),
            dma((1,)), dma((n,)), dma((1,)), dma((n, ny - 1)), dma((1,)), dma((groups,)),
            dma((1,)), dma((groups,)), dma((1,)), dma((n, ny - 1)), dma((1,)), dma((1,)),
            dma((1,)), dma((1,)),
        ]
        near = pl.BlockSpec(memory_space=pltpu.VMEM)
        far = pl.BlockSpec(memory_space=pl.ANY)
        return pl.pallas_call(
            functools.partial(layer_kernel, n, nt, cap, size),
            out_shape=pltpu.VMEM((rows_here, width), BF16),
            in_specs=[far] * 16,
            out_specs=near,
            scratch_shapes=scratch,
            compiler_params=pltpu.CompilerParams(
                collective_id=0, has_side_effects=True, vmem_limit_bytes=64_000_000
            ),
            name="layer",
        )(*given)

    return jax.shard_map(
        body,
        mesh=mesh,
        in_specs=(
            P(("sp", "tp"), None), P("sp", "tp"), P("sp", "tp"), P("sp", "tp"), P("sp", None),
            P(None, "tp"), P("tp"), P("sp", "tp"), P(), P("tp", None), P(), P("sp", None),
            P("sp", None), P("sp", None, "tp"), P("sp", None, "tp"), P("sp", "tp", None),
        ),
        out_specs=P(("sp", "tp"), None),
        check_vma=False,
    )
```

```python
import functools

import jax
import jax.numpy as jnp
from jax import lax
from jax.experimental import pallas as pl
from jax.experimental.pallas import tpu as pltpu
from jax.sharding import PartitionSpec as P

HK = 256
HV = 512
TOP = 2
PIECES = 4
BLK = 128
TEMPER = 16.0
EPSILON = 1e-06
HIGHEST = lax.Precision.HIGHEST
MESH = pl.DeviceIdType.MESH
F32 = jnp.float32
BF16 = jnp.bfloat16


def mm(a, b, ca, cb, precision=None):
    return lax.dot_general(
        a, b, (((ca,), (cb,)), ((), ())), preferred_element_type=F32, precision=precision
    )


def remote(src, dst, send, recv, target):
    return pltpu.make_async_remote_copy(
        src_ref=src, dst_ref=dst, send_sem=send, recv_sem=recv, device_id=target, device_id_type=MESH
    )


def layer_kernel(
    n, nt, cap, size,
    stream_in, q_in, k_in, v_in, low_in, mat_in, bias_in, shift_in, gain_in, wout, fgain_in, routes_in,
    rweights_in, wgate, wup, wdown,
    out,
    stream, q, k, v, low, mat, bias, shift, gain, fgain, routes, rweights,
    ins, prior, sbuf, rbuf, cbuf, carry, tsend, trecv, dec, decall, acc, qs,
    wo, wgud, wt, mixed,
    scols, prod, p1, ph, p2, mid, selt, wcomb, sca, scb,
    fb, rows, gates, hiddens, pb, r4, hy, r6, hb, r5, outc, fin,
    wsem, lsem, sa, ra, sd, rd, sb, rb, stt, rtt, sst, rst, sp1, rp1, sp2, rp2, ssc, rsc,
    sx, rx, sy, ry, sxc, rxc, s4, q4, s6, q6, s5, q5, sf, rf,
):
    me = lax.axis_index("sp")
    t = lax.axis_index("tp")
    y = t // 2
    c = lax.rem(t, 2)
    ny = nt // 2
    mine, team, teams = lax.rem(me, size), me // size, n // size
    first_one = team * size
    partner = {"tp": 2 * y + 1 - c}
    length = q.shape[0]
    heads = q.shape[1] // HK
    blocks = length // BLK
    width = stream.shape[1]
    rows_here = stream.shape[0]
    cw = width // nt
    tile = min(256, cw)
    sides = [slice(f * tile, (f + 1) * tile) for f in range(cw // tile)]
    high = HV // size
    piece = max(16, high // PIECES)
    pieces = [slice(a, a + piece) for a in range(0, high, piece)]

    def send(*args):
        remote(*args).start()

    def arrived(ref, semaphore):
        remote(ref, ref, semaphore, semaphore, partner).wait_recv()

    def departed(ref, semaphore):
        remote(ref, ref, semaphore, semaphore, partner).wait_send()

    def columns(p, f=0, wide=tile):
        return pl.ds(pl.multiple_of(p * cw + f * tile, tile), wide)

    total_devices = n * nt
    rank = me * nt + t
    barrier = pltpu.get_barrier_semaphore()

    @pl.loop(1, total_devices)
    def _(i):
        other = lax.rem(rank + i, total_devices)
        there = {"sp": other // nt, "tp": lax.rem(other, nt)}
        pl.semaphore_signal(barrier, inc=1, device_id=there, device_id_type=MESH)

    loads = [
        pltpu.make_async_copy(source, target, lsem.at[i])
        for i, (source, target) in enumerate((
            (low_in, low), (mat_in, mat), (bias_in, bias), (shift_in, shift), (k_in, k), (v_in, v),
            (stream_in, stream), (q_in, q), (routes_in, routes), (rweights_in, rweights), (gain_in, gain),
            (fgain_in, fgain),
        ))
    ]
    for load in loads:
        load.start()
    load_out = pltpu.make_async_copy(wout, wo, wsem.at[0])
    load_out.start()
    for i, weight in enumerate((wgate, wup, wdown)):
        pltpu.make_async_copy(weight.at[0], wgud.at[i], wsem.at[1]).start()

    row_id = lax.broadcasted_iota(jnp.int32, (BLK, BLK), 0)
    col_id = lax.broadcasted_iota(jnp.int32, (BLK, BLK), 1)
    causal = row_id >= col_id
    tril = causal.astype(F32)

    for load in loads[:4]:
        load.wait()
    shifts = shift[...].T

    for h in range(heads):
        ks, vs = slice(h * HK, (h + 1) * HK), slice(h * HV, (h + 1) * HV)
        pre = mm(low[...], mat[:, ks], 0, 0) + bias[:, ks]
        logged = (jnp.minimum(pre, 0.0) - jnp.log1p(jnp.exp(-jnp.abs(pre)))) / TEMPER + shifts[:, h : h + 1]
        if h == 0:
            for load in loads[4:6]:
                load.wait()
        whole = None
        state = None
        for b in range(blocks):
            at = slice(b * BLK, (b + 1) * BLK)
            inside = mm(tril, logged[at], 1, 0, HIGHEST)
            ins[at, ks] = inside
            last = inside[BLK - 1 : BLK, :]
            whole = last if whole is None else whole + last
            end = (k[at, ks].astype(F32) * jnp.exp(last - inside)).astype(BF16)
            added = mm(v[at, vs], end, 0, 0)
            state = added if state is None else state * jnp.exp(last) + added
            if b < blocks - 1:
                prior[b, :, ks] = state.astype(BF16)
        sbuf[h] = state.astype(BF16).reshape(size, HV // size, HK)
        dec[h] = jnp.exp(whole)
        if h == 0:
            pl.semaphore_wait(barrier, total_devices - 1)
        for i in range(1, size):
            to = lax.rem(mine + i, size)
            send(dec.at[h], decall.at[h, mine], sd.at[0], rd.at[h], {"sp": first_one + to})
        for p, part in enumerate(pieces):
            for i in range(1, size):
                to = lax.rem(mine + i, size)
                send(
                    sbuf.at[h, to, part], rbuf.at[h, mine, part], sa.at[0], ra.at[h, p], {"sp": first_one + to}
                )
        rbuf[h, mine] = sbuf[h, mine]
        decall[h, mine] = dec[h]

    for load in loads[6:]:
        load.wait()
    for i in range(1, nt):
        to = lax.rem(t + i, nt)
        send(stream.at[:, columns(to, 0, cw)], scols.at[t], sst.at[0], rst.at[0], {"tp": to})
    scols[t] = stream[:, columns(t, 0, cw)]

    turns = [(j, slice(a, a + 256)) for j in range(2) for a in range(0, width, 256)]
    onward = {"sp": lax.rem(me + size, n)}
    for h in range(heads):
        ks, vs = slice(h * HK, (h + 1) * HK), slice(h * HV, (h + 1) * HV)
        arrived(decall.at[h, 0 : size - 1], rd.at[h])
        for p, part in enumerate(pieces):
            arrived(rbuf.at[h, 0 : size - 1, part], ra.at[h, p])
            link = remote(tsend.at[h, part], trecv.at[h, part], stt.at[0], rtt.at[h, p], onward)

            @pl.when(team > 0)
            def _():
                link.wait_recv()

            @pl.when(team == 0)
            def _():
                trecv[h, part] = jnp.zeros_like(trecv[h, part])

            total = trecv[h, part].astype(F32)
            for j in range(size):
                cbuf[h, j, part] = total.astype(BF16)
                total = total * decall[h, j] + rbuf[h, j, part].astype(F32)

            @pl.when(team < teams - 1)
            def _():
                tsend[h, part] = total.astype(BF16)
                link.start()

            for i in range(1, size):
                j = lax.rem(mine + i, size)
                send(cbuf.at[h, j, part], carry.at[h, mine, part], sb.at[0], rb.at[h], {"sp": first_one + j})
        carry[h, mine] = cbuf[h, mine]

        passed = None
        for b in range(blocks):
            at = slice(b * BLK, (b + 1) * BLK)
            inside = ins[at, ks]
            last = inside[BLK - 1 : BLK, :]
            centre = last * 0.5
            qf = q[at, ks].astype(F32) * HK ** (-0.5)
            sq = (qf * jnp.exp(inside - centre)).astype(BF16)
            sk = (k[at, ks].astype(F32) * jnp.exp(centre - inside)).astype(BF16)
            scores = jnp.where(causal, mm(sq, sk, 1, 1), 0.0).astype(BF16)
            local = mm(scores, v[at, vs], 1, 0)
            full = inside if passed is None else inside + passed
            qs[at, ks] = (qf * jnp.exp(full)).astype(BF16)
            if b > 0:
                local = local + mm((qf * jnp.exp(inside)).astype(BF16), prior[b - 1, :, ks], 1, 1)
            passed = last if passed is None else passed + last
            acc[at, vs] = local
        if h == 0:
            pltpu.make_async_copy(wgud, wgud, wsem.at[1]).wait()
        if h < max(1, heads - 1):
            for j, at in turns[h :: max(1, heads - 1)]:
                wt[j, at, :] = wgud[j, :, at].T
        if h == min(1, heads - 1):
            lane = lax.broadcasted_iota(jnp.int32, (length, n), 1).astype(F32)
            named = routes[...].astype(F32).T
            shares = rweights[...].T
            first_named = (named[:, 0:1] == lane).astype(F32)
            second_named = (named[:, 1:2] == lane).astype(F32)
            earlier = (
                lax.broadcasted_iota(jnp.int32, (length, length), 0)
                > lax.broadcasted_iota(jnp.int32, (length, length), 1)
            ).astype(BF16)
            counts = mm(earlier, (first_named + second_named).astype(BF16), 1, 0)
            slot_lane = lax.broadcasted_iota(jnp.int32, (length, n * cap), 1).astype(F32)
            chosen = jnp.zeros((length, n * cap), F32)
            weighted = jnp.zeros((length, n * cap), F32)
            for j, mask in enumerate((first_named, second_named)):
                rank = jnp.sum(counts * mask, axis=1, keepdims=True)
                place = jnp.where(rank < cap, named[:, j : j + 1] * cap + rank, -1.0)
                hit = place == slot_lane
                chosen = chosen + jnp.where(hit, 1.0, 0.0)
                weighted = weighted + jnp.where(hit, shares[:, j : j + 1], 0.0)
            selt[...] = chosen.T.astype(BF16)
            wcomb[...] = weighted.astype(BF16)
            sca[...] = jnp.zeros_like(sca)


    for h in range(heads):
        ks, vs = slice(h * HK, (h + 1) * HK), slice(h * HV, (h + 1) * HV)
        arrived(carry.at[h, 0 : size - 1], rb.at[h])
        x = acc[:, vs] + mm(qs[:, ks], carry[h].reshape(HV, HK), 1, 1)
        scale = lax.rsqrt(jnp.mean(x * x, axis=-1, keepdims=True) + EPSILON)
        mixed[:, vs] = (x * scale * gain[...]).astype(BF16)

    load_out.wait()

    def first(to, f):
        at = sides[f]
        return remote(
            prod.at[to, 1 - c, :, at], p1.at[to, :, at], sp1.at[0], rp1.at[f, to], partner
        )

    def second(to, slot, f):
        at = sides[f]
        return remote(
            ph.at[to, :, at], p2.at[slot, :, at], sp2.at[0], rp2.at[f, slot], {"tp": 2 * to + c}
        )

    def project(to, core, f):
        prod[to, core, :, sides[f]] = mm(mixed[...], wo[:, columns(2 * to + core, f)], 1, 0).astype(BF16)

    for i in range(1, ny + 1):
        to = lax.rem(y + i, ny)
        for f in range(len(sides)):
            project(to, 1 - c, f)
            first(to, f).start()
        for f in range(len(sides)):
            project(to, c, f)
        if i < ny:
            for f, at in enumerate(sides):
                first(to, f).wait_recv()
                ph[to, :, at] = (prod[to, c, :, at].astype(F32) + p1[to, :, at].astype(F32)).astype(BF16)
                second(to, y, f).start()

    arrived(scols.at[0 : nt - 1], rst.at[0])
    square = jnp.zeros((length, 1), F32)
    for f, at in enumerate(sides):
        first(y, f).wait_recv()
        total = prod[y, c, :, at].astype(F32) + p1[y, :, at].astype(F32)
        for i in range(1, ny):
            to = lax.rem(y + i, ny)
            second(to, to, f).wait_recv()
            total = total + p2[to, :, at].astype(F32)
        x = scols[:, :, at].reshape(length, tile).astype(F32) + total
        mid[:, at] = x
        square = square + jnp.sum(x * x, axis=1, keepdims=True)
        picked = mm(selt[...], (x * fgain[:, columns(t, f)]).astype(BF16), 1, 0)
        fb[:, :, at] = picked.astype(BF16).reshape(n, cap, tile)
        for i in range(1, n):
            to = lax.rem(me + i, n)
            send(fb.at[to, :, at], rows.at[me, t, :, at], sx.at[0], rx.at[me], {"sp": to})
        if f == len(sides) - 1:
            row = jnp.broadcast_to(square, (length, 128)).T[0:8, :]
            upper = row.astype(BF16).astype(F32)
            middle = (row - upper).astype(BF16).astype(F32)
            line = lax.broadcasted_iota(jnp.int32, (8, length), 0)
            parts = jnp.where(line == 0, upper, jnp.where(line == 1, middle, jnp.where(line == 2, row - upper - middle, 0.0)))
            slot_squares = jnp.sum(mm(parts.astype(BF16), selt[...], 1, 1), axis=0, keepdims=True)
            for e in range(n):
                sca[e, :, 0:cap] = slot_squares[:, e * cap : (e + 1) * cap]
            for i in range(n):
                to = lax.rem(me + i, n)
                for j in range(0 if i else 1, nt):
                    send(
                        sca.at[to], scb.at[me * nt + t], ssc.at[0], rsc.at[0], {"sp": to, "tp": lax.rem(t + j, nt)}
                    )
            scb[me * nt + t] = sca[me]

    step = max(1, min(n, 256 // cap))
    groups = [range(a, a + step) for a in range(0, n, step)]
    if step > 1:
        first_half = groups[-1][: step // 2]
        groups = groups[:-1] + [first_half, groups[-1][step // 2 :]]

    def group_of(i):
        return next(g for g, group in enumerate(groups) if i in group)

    def group_at(i):
        g = 0
        for group in groups[1:]:
            g = g + (i >= group[0]).astype(jnp.int32)
        return g

    def forward(i, g):
        block = rows.at[i, t]
        for d in range(1, ny):
            send(block, rows.at[i, t], sy.at[0], ry.at[i, d - 1], {"tp": 2 * lax.rem(y + d, ny) + c})
        send(block, rows.at[i, t], sxc.at[0], rxc.at[g], partner)

    def pass_on(i):
        @pl.when(i // size != team)
        def _():
            arrived(rows.at[i, t], rx.at[i])
            forward(i, group_of(i))

    def pass_over(i):
        for d in range(1, ny):
            other = lax.rem(y + ny - d, ny)
            block = rows.at[i, 2 * other + c]
            arrived(block, ry.at[i, d - 1])
            send(block, block, sxc.at[0], rxc.at[group_of(i)], partner)

    def experts(g):
        group = groups[g]
        span = slice(group[0], group[-1] + 1)
        size_here = len(group) * cap
        arrived(rows.at[span, 0:ny], rxc.at[g])
        parts = [rows[span, p].reshape(size_here, cw) for p in range(nt)]
        gates[0:size_here] = mm(jnp.concatenate(parts, axis=1), wt[0], 1, 0)
        yield
        parts = [rows[span, p].reshape(size_here, cw) for p in range(nt)]
        lifted = mm(jnp.concatenate(parts, axis=1), wt[1], 1, 0)
        if g == 0:
            arrived(scb.at[0 : n * nt - 1], rsc.at[0])
        scales = []
        for i in group:
            total = jnp.sum(scb[i * nt : (i + 1) * nt], axis=0)
            line = lax.rsqrt(total / width + EPSILON)
            scales.append(jnp.broadcast_to(line, (8, 128)).T[0:cap, 0:1])
        scale = jnp.concatenate(scales, axis=0)
        lifted = lifted * scale
        gated = gates[0:size_here] * scale
        hiddens[0:size_here] = (gated * jax.nn.sigmoid(gated) * lifted).astype(BF16)
        yield
        for core in (1 - c, c):
            for d in range(ny):
                piece = mm(hiddens[0:size_here], wgud[2, :, columns(2 * d + core, 0, cw)], 1, 0).astype(BF16)
                pb[span, d, core] = piece.reshape(len(group), cap, cw)
            if core is not c:
                for i in group:
                    for d in range(ny):
                        send(pb.at[i, d, core], r4.at[i, d], s4.at[0], q4.at[g], partner)
            yield

    def over_core(i):
        for d in range(1, ny):
            other = lax.rem(y + d, ny)
            hy[i, other] = (pb[i, other, c].astype(F32) + r4[i, other].astype(F32)).astype(BF16)
            send(hy.at[i, other], r6.at[i, d], s6.at[0], q6.at[i, d - 1], {"tp": 2 * other + c})

    def over_y(i):
        both = pb[i, y, c].astype(F32) + r4[i, y].astype(F32)
        for d in range(1, ny):
            arrived(r6.at[i, d], q6.at[i, d - 1])
            both = both + r6[i, d].astype(F32)
        hb[i] = both.astype(BF16)

        @pl.when(i == me)
        def _():
            r5[me] = hb[i]

        @pl.when(i != me)
        def _():
            send(hb.at[i], r5.at[me], s5.at[0], q5.at[0], {"sp": i})


    work, computed, returned = [], [], []

    def back(g):
        arrived(r4.at[groups[g][0] : groups[g][-1] + 1], q4.at[g])
        for i in groups[g]:
            over_core(i)
            returned.append(i)

    def one_stage():
        if work:
            if computed:
                back(computed.pop(0))
            g, stages = work[0]
            next(stages)
            if g_left[g] == 1:
                work.pop(0)
                computed.append(g)
            g_left[g] -= 1

    g_left = [4] * len(groups)
    rows[me, t] = fb[me]
    forward(me, group_at(me))
    for i in range(1, size):
        mate = first_one + lax.rem(mine + i, size)
        arrived(rows.at[mate, t], rx.at[mate])
        forward(mate, group_at(mate))
    lag = 3
    for i in range(n + lag):
        if i < n:
            pass_on(i)
        one_stage()
        if i >= lag:
            pass_over(i - lag)
            for g, group in enumerate(groups):
                if group[-1] == i - lag:
                    work.append((g, experts(g)))
        one_stage()
    while work:
        one_stage()
    for g in computed:
        back(g)
    for i in returned:
        over_y(i)
    arrived(r5.at[0 : n - 1], q5.at[0])

    finished = mid[...] + mm(wcomb[...], r5[...].reshape(n * cap, cw), 1, 0)
    outc[...] = finished.astype(BF16).reshape(nt, rows_here, cw)
    for i in range(1, nt):
        p = lax.rem(t + i, nt)
        send(outc.at[p], fin.at[t], sf.at[0], rf.at[0], {"tp": p})
    fin[t] = outc[t]
    arrived(fin.at[0 : nt - 1], rf.at[0])
    for p in range(nt):
        out[:, p * cw : (p + 1) * cw] = fin[p]
    departed(decall.at[:, 0 : size - 1], sd.at[0])
    departed(sbuf.at[:, 0 : size - 1], sa.at[0])
    departed(cbuf.at[:, 0 : size - 1], sb.at[0])
    departed(scols.at[0 : nt - 1], sst.at[0])
    departed(p1, sp1.at[0])
    departed(ph.at[0 : ny - 1], sp2.at[0])
    departed(scb.at[0 : n * nt - 1], ssc.at[0])
    departed(fb.at[0 : n - 1], sx.at[0])
    departed(hy.at[:, 0 : ny - 1], sy.at[0])
    departed(r4, sxc.at[0])
    departed(r4, s4.at[0])
    departed(hy.at[:, 0 : ny - 1], s6.at[0])
    departed(hb.at[0 : n - 1], s5.at[0])
    departed(outc.at[0 : nt - 1], sf.at[0])

    @pl.when(team < teams - 1)
    def _():
        departed(tsend, stt.at[0])


def solution(mesh):
    n, nt = mesh.shape["sp"], mesh.shape["tp"]
    ny = nt // 2

    def body(
        stream_in, queries, key_rows, values, decay_low, decay_matrix, decay_bias, decay_shift,
        head_gain, output_matrix, feed_gain, routes, route_weights, expert_gate, specialist_widen,
        expert_down,
    ):
        length, keys = queries.shape
        vals = values.shape[1]
        rows_here, width = stream_in.shape
        hidden = expert_gate.shape[2]
        cap = nt * max(1, TOP * length // (n * nt))
        cw = width // nt
        sides = cw // min(256, cw)
        step = max(1, min(n, 256 // cap))
        groups = n // step + 1
        size = next(x for x in ((4, 2, 1) if n > 8 else (2, 1)) if n % x == 0)
        pieces = (HV // size) // max(16, HV // size // PIECES)
        heads = keys // HK
        blocks = length // BLK
        vm = pltpu.VMEM
        dma = pltpu.SemaphoreType.DMA
        given = [
            stream_in, queries, key_rows, values, decay_low.T, decay_matrix, decay_bias.reshape(1, -1),
            decay_shift.T, head_gain.reshape(1, -1), output_matrix, feed_gain.reshape(1, -1), routes.T,
            route_weights.T, expert_gate.swapaxes(1, 2), specialist_widen.swapaxes(1, 2), expert_down,
        ]
        scratch = [
            *[vm(given[i].shape, given[i].dtype) for i in (0, 1, 2, 3, 4, 5, 6, 7, 8, 10, 11, 12)],
            vm((length, keys), F32), vm((max(1, blocks - 1), HV, keys), BF16),
            *[vm((heads, size, HV // size, HK), BF16)] * 4,
            *[vm((heads, HV // size, HK), BF16)] * 2,
            vm((heads, 1, HK), F32), vm((heads, size, 1, HK), F32),
            vm((length, vals), F32), vm((length, keys), BF16),
            vm(output_matrix.shape, BF16), vm((3, hidden, width), BF16), vm((2, width, hidden), BF16), vm((length, vals), BF16),
            vm((nt, rows_here, cw), BF16), vm((ny, 2, length, cw), BF16), *[vm((ny, length, cw), BF16)] * 3,
            vm((length, cw), F32),
            vm((n * cap, length), BF16), vm((length, n * cap), BF16),
            vm((n, 1, 128), F32), vm((n * nt, 1, 128), F32),
            vm((n, cap, cw), BF16), vm((n, nt, cap, cw), BF16),
            vm((step * cap, hidden), F32), vm((step * cap, hidden), BF16),
            vm((n, ny, 2, cap, cw), BF16), *[vm((n, ny, cap, cw), BF16)] * 3,
            vm((n, cap, cw), BF16), vm((n, cap, cw), BF16),
            vm((nt, rows_here, cw), BF16), vm((nt, rows_here, cw), BF16),
            dma((2,)), dma((12,)),
            dma((1,)), dma((heads, pieces)), dma((1,)), dma((heads,)),
            dma((1,)), dma((heads,)), dma((1,)), dma((heads, pieces)),
            dma((1,)), dma((1,)), dma((1,)), dma((sides, ny)), dma((1,)), dma((sides, ny)),
            dma((1,)), dma((1,)),
            dma((1,)), dma((n,)), dma((1,)), dma((n, ny - 1)), dma((1,)), dma((groups,)),
            dma((1,)), dma((groups,)), dma((1,)), dma((n, ny - 1)), dma((1,)), dma((1,)),
            dma((1,)), dma((1,)),
        ]
        near = pl.BlockSpec(memory_space=pltpu.VMEM)
        far = pl.BlockSpec(memory_space=pl.ANY)
        return pl.pallas_call(
            functools.partial(layer_kernel, n, nt, cap, size),
            out_shape=pltpu.VMEM((rows_here, width), BF16),
            in_specs=[far] * 16,
            out_specs=near,
            scratch_shapes=scratch,
            compiler_params=pltpu.CompilerParams(
                collective_id=0, has_side_effects=True, vmem_limit_bytes=64_000_000
            ),
            name="layer",
        )(*given)

    return jax.shard_map(
        body,
        mesh=mesh,
        in_specs=(
            P(("sp", "tp"), None), P("sp", "tp"), P("sp", "tp"), P("sp", "tp"), P("sp", None),
            P(None, "tp"), P("tp"), P("sp", "tp"), P(), P("tp", None), P(), P("sp", None),
            P("sp", None), P("sp", None, "tp"), P("sp", None, "tp"), P("sp", "tp", None),
        ),
        out_specs=P(("sp", "tp"), None),
        check_vma=False,
    )
```
